128 devices in a mesh: sp: 16 (over z, y), dp: 8 (over x, core).
Axes of the slice: x: 4, y: 4, z: 4, core: 2. Of those that a mesh axis runs over, the one named last changes fastest.
Arguments:
- hidden_in: bfloat16 [2048, 16, 2048], P('sp', 'dp'), may hold values from -6 to 6
- query_act: bfloat16 [2048, 16, 1024], P('sp', 'dp'), may hold values from -4 to 4
- key_act: bfloat16 [2048, 16, 1024], P('sp', 'dp'), may hold values from -4 to 4
- gate_act: bfloat16 [2048, 16, 1024], P('sp', 'dp'), may hold values from -4 to 4
- decay_bias: float32 [1024], replicated, as said below
- value_weight: bfloat16 [2048, 2048], P('dp'), may hold values from -0.125 to 0.125
- out_grad: bfloat16 [2048, 16, 2048], P('sp', 'dp'), may hold values from -0.29882812 to 0.29882812
Outputs:
- hidden_grad: bfloat16 [2048, 16, 2048], P('sp', 'dp')
- query_grad: bfloat16 [2048, 16, 1024], P('sp', 'dp')
- key_grad: bfloat16 [2048, 16, 1024], P('sp', 'dp')
- gate_grad: bfloat16 [2048, 16, 1024], P('sp', 'dp')
- weight_grad: float32 [2048, 2048], P('dp', 'sp')
The draws below stay inside these ranges and needn't reach their ends.
Inputs may be any that keep to these rules, and one draw needn't show every extreme that they name: `decay_bias`: every offset is at least -1 and at most 1 plus the natural logarithm of 128.
All inputs are finite; a program needn't handle non-finite values.
Results may differ from the reference program's by a relative error of at most 0.018.
Values may be sent and summed in bfloat16 or wider, within the bound.
No kernel may reach another device: no remote copies, remote signals or barrier semaphores. Data moves between devices by JAX's collectives and lax.ppermute only.
A program may use at most 128 MiB of HBM per device.

```python
import math
import jax
import jax.numpy as jnp
from jax import lax

D = 2048
HEADS = 8
DK = 128
DV = 256
BLK = 128
LENGTH = 2048
BATCH = 16


def draw_gate_act(key, part):
    noise_key, factor_key = jax.random.split(jax.random.fold_in(key, 11))
    blocks = LENGTH // BLK
    factor = jnp.exp(jax.random.uniform(factor_key, (blocks, 1, BATCH, 1), jnp.float32, math.log(0.3), math.log(1.2)))
    noise = jnp.clip(jax.random.normal(noise_key, (blocks, BLK, BATCH, HEADS * DK), jnp.float32), -3.3, 3.3)
    return (noise * factor).reshape(LENGTH, BATCH, HEADS * DK).astype(jnp.bfloat16)


def draw_decay_bias(key, part):
    ranking_key, spread_key = jax.random.split(jax.random.fold_in(key, 23))
    ranking = jax.random.permutation(ranking_key, HEADS)
    fast_count = HEADS // 2
    fast_head = ranking < fast_count
    jitter = jax.random.uniform(spread_key, (HEADS, DK), jnp.float32, -0.5, 0.5)
    slow_bias = 0.5 + math.log(LENGTH / 16.0) + jitter
    return jnp.where(fast_head[:, None], 2.0 * jitter, slow_bias).reshape(HEADS * DK)


def shard_levels(own_key, shape, cuts, smallest, largest):
    level = 1.0
    for dim, shards_of in cuts:
        heights = jax.random.uniform(jax.random.fold_in(jax.random.fold_in(own_key, 6), dim), (shards_of,), jnp.float32, smallest / len(cuts), largest / len(cuts))
        level = level * jnp.repeat(jnp.exp(heights), shape[dim] // shards_of).reshape((-1,) + (1,) * (len(shape) - 1 - dim))
    return level


def normal_values(stream_key, extent, deviation, limit, shards=(), kind=jnp.bfloat16):
    array = jax.random.normal(stream_key, extent, jnp.float32) * deviation
    if len(shards) > 0:
        array = shard_levels(stream_key, extent, shards, -0.22, 0.18) * array
    return jnp.clip(array, min=-limit, max=limit).astype(kind)


def setup_inputs(seed: int = 0) -> dict:
    key_list = jax.random.split(jax.random.key(seed), 8)
    hidden_in = normal_values(key_list[0], (LENGTH, BATCH, D), 1.0, 6.0, ((0, 16), (1, 8)))
    query_act = normal_values(key_list[1], (LENGTH, BATCH, HEADS * DK), 1.0, 4.0, ((0, 16), (1, 8)))
    key_act = normal_values(key_list[2], (LENGTH, BATCH, HEADS * DK), 1.0, 4.0, ((0, 16), (1, 8)))
    gate_act = draw_gate_act(jax.random.fold_in(key_list[7], 71), 0)
    decay_bias = draw_decay_bias(jax.random.fold_in(key_list[7], 71), 0)
    value_weight = normal_values(key_list[5], (D, HEADS * DV), D ** -0.5, 0.125, ((0, 8),))
    out_grad = normal_values(key_list[6], (LENGTH, BATCH, HEADS * DV), 0.05, 0.29882812, ((0, 16), (1, 8)))
    return dict(hidden_in=hidden_in, query_act=query_act, key_act=key_act, gate_act=gate_act, decay_bias=decay_bias, value_weight=value_weight, out_grad=out_grad)


softness = 16.0

def combine_states(earlier, latter):
    return (earlier[0] * latter[0], latter[0][..., None] * earlier[1] + latter[1])

def block_forward(query_rows, key_rows, value_rows, gate_rows, bias_row):
    length, width_key = query_rows.shape
    width_value = value_rows.shape[1]
    blocks = length // BLK
    highest = lax.Precision.HIGHEST
    query_blocks = (query_rows.astype(jnp.float32) * width_key ** (-0.5)).reshape(blocks, BLK, width_key)
    key_blocks = key_rows.astype(jnp.float32).reshape(blocks, BLK, width_key)
    value_blocks = value_rows.astype(jnp.float32).reshape(blocks, BLK, width_value)
    log_decay = jax.nn.log_sigmoid(gate_rows.astype(jnp.float32) + bias_row) / softness
    cumulative = jnp.cumsum(log_decay.reshape(blocks, BLK, width_key), axis=1)
    final_log = cumulative[:, -1:, :]
    query_decayed = query_blocks * jnp.exp(cumulative)
    key_inverse = key_blocks * jnp.exp(-cumulative)
    scores = jnp.einsum('ncd,nsd->ncs', query_decayed, key_inverse, precision=highest)
    lower_mask = jnp.tril(jnp.ones((BLK, BLK), jnp.float32))
    output = jnp.einsum('ncs,nsv->ncv', scores * lower_mask, value_blocks, precision=highest)
    state_delta = jnp.einsum('ncd,ncv->ndv', key_blocks * jnp.exp(final_log - cumulative), value_blocks, precision=highest)
    decay_total = jnp.exp(final_log[:, 0, :])
    decays, running = lax.associative_scan(combine_states, (decay_total, state_delta))
    carried = jnp.concatenate([jnp.zeros((1, width_key, width_value), jnp.float32), running[:-1]], axis=0)
    output = output + jnp.einsum('ncd,ndv->ncv', query_decayed, carried, precision=highest)
    return output.reshape(length, width_value)

def item_backward(query_rows, key_rows, value_rows, gate_rows, bias_row, grad_rows):

    def forward(query_in, key_in, value_in, gate_in):
        return block_forward(query_in, key_in, value_in, gate_in, bias_row)
    output, pullback = jax.vjp(forward, query_rows, key_rows, value_rows, gate_rows)
    return pullback(grad_rows.astype(jnp.float32))

def to_items(source, width):
    return jnp.transpose(source.reshape(LENGTH, BATCH * HEADS, width), (1, 0, 2))

def from_items(source, width):
    return jnp.transpose(source, (1, 0, 2)).reshape(LENGTH, BATCH, HEADS * width)

def run_item(packed):
    return item_backward(*packed)

def reference(hidden_in, query_act, key_act, gate_act, decay_bias, value_weight, out_grad):
    flat_in = hidden_in.reshape(LENGTH * BATCH, D)
    values_act = jnp.dot(flat_in, value_weight, preferred_element_type=jnp.float32).astype(jnp.bfloat16)
    values_act = values_act.reshape(LENGTH, BATCH, HEADS * DV)
    biases = jnp.tile(decay_bias.reshape(HEADS, DK), (BATCH, 1))
    grads = lax.map(run_item, (to_items(query_act, DK), to_items(key_act, DK), to_items(values_act, DV), to_items(gate_act, DK), biases, to_items(out_grad, DV)))
    value_grad = from_items(grads[2], DV).reshape(LENGTH * BATCH, HEADS * DV)
    hidden_grad = jnp.dot(value_grad, value_weight.T, preferred_element_type=jnp.float32).astype(jnp.bfloat16)
    weight_grad = jnp.dot(flat_in.T, value_grad, preferred_element_type=jnp.float32)
    return (hidden_grad.reshape(LENGTH, BATCH, D), from_items(grads[0], DK), from_items(grads[1], DK), from_items(grads[3], DK), weight_grad)
```

```python
import functools

import jax
import jax.numpy as jnp
from jax import lax
from jax.experimental import pallas as pl
from jax.experimental.pallas import tpu as pltpu
from jax.sharding import PartitionSpec as P

HEADS = 8
DK = 128
DV = 256
BLK = 128
EXTRA = 16
SOFTNESS = 16.0
SCALE = DK**-0.5
F32 = jnp.float32
BF16 = jnp.bfloat16

NN = (((1,), (0,)), ((), ()))
NT = (((1,), (1,)), ((), ()))
TN = (((0,), (0,)), ((), ()))


def dot(a, b, dims):
    return lax.dot_general(a, b, dims, preferred_element_type=F32)


def split2(x):
    hi = x.astype(BF16)
    lo = (x - hi.astype(F32)).astype(BF16)
    return hi, lo


def iota_pair(shape):
    return (
        lax.broadcasted_iota(jnp.int32, shape, 0),
        lax.broadcasted_iota(jnp.int32, shape, 1),
    )


def cost(flops, moved):
    return pl.CostEstimate(flops=flops, bytes_accessed=moved, transcendentals=0)


def params():
    return pltpu.CompilerParams(dimension_semantics=("arbitrary",))


def decay_kernel(pair, q_ref, g_ref, bias_ref, do_ref, delta_ref, cum_ref):
    row, col = iota_pair((BLK, BLK))
    lower = (row >= col).astype(BF16)
    for s in range(2):
        for j in range(pair):
            keys = slice(j * DK, (j + 1) * DK)
            x = g_ref[s, :, keys].astype(F32) + bias_ref[:, keys]
            log_decay = (jnp.minimum(x, 0.0) - jnp.log1p(jnp.exp(-jnp.abs(x)))) / SOFTNESS
            hi, lo = split2(log_decay)
            cum = dot(lower, hi, NN) + dot(lower, lo, NN)
            cum_ref[s, :, keys] = cum
            q_dec = (q_ref[s, :, keys].astype(F32) * SCALE * jnp.exp(cum)).astype(BF16)
            delta = dot(do_ref[s, :, j * DV : (j + 1) * DV], q_dec, TN)
            delta_ref[s, j, :DV, :] = delta.astype(BF16)
            last = cum[BLK - 1 : BLK, :]
            one, two = split2(last)
            three = (last - one.astype(F32) - two.astype(F32)).astype(BF16)
            rows = lax.broadcasted_iota(jnp.int32, (EXTRA, DK), 0)
            tail = jnp.where(
                rows == 0,
                one.astype(F32),
                jnp.where(rows == 1, two.astype(F32), three.astype(F32)),
            )
            delta_ref[s, j, DV:, :] = tail.astype(BF16)


def intra_kernel(pair, q_ref, k_ref, cum_ref, do_ref, dv_ref):
    row, col = iota_pair((BLK, BLK))
    for s in range(2):
        for j in range(pair):
            keys = slice(j * DK, (j + 1) * DK)
            vals = slice(j * DV, (j + 1) * DV)
            cum = cum_ref[s, :, keys]
            q_dec = (q_ref[s, :, keys].astype(F32) * SCALE * jnp.exp(cum)).astype(BF16)
            k_inv = (k_ref[s, :, keys].astype(F32) * jnp.exp(-cum)).astype(BF16)
            scores = dot(q_dec, k_inv, NT)
            scores = jnp.where(row >= col, scores, 0.0).astype(BF16)
            dv_ref[s, :, vals] = dot(scores, do_ref[s, :, vals], TN)


def scan_kernel(blocks, reverse, rx_ref, last_ref, out_ref):
    state = jnp.zeros((DV, DK), F32)
    order = range(blocks - 1, -1, -1) if reverse else range(blocks)
    for b in order:
        out_ref[b] = state.astype(BF16)
        tail = last_ref[b].astype(F32)
        decay = jnp.exp(tail[0:1] + tail[1:2] + tail[2:3])
        state = state * decay + rx_ref[b, :DV, :].astype(F32)


def value_grad_kernel(pair, k_ref, cum_ref, dstate_ref, dv_in_ref, dv_ref):
    for s in range(2):
        for j in range(pair):
            keys = slice(j * DK, (j + 1) * DK)
            vals = slice(j * DV, (j + 1) * DV)
            cum = cum_ref[s, :, keys]
            last = cum[BLK - 1 : BLK, :]
            k_dec = (k_ref[s, :, keys].astype(F32) * jnp.exp(last - cum)).astype(BF16)
            inter = dot(k_dec, dstate_ref[s, j], NT)
            dv_ref[s, :, vals] = (dv_in_ref[s, :, vals] + inter).astype(BF16)


def project_kernel(h_ref, w_ref, k_ref, cum_ref, v_ref, delta_ref):
    v_all = dot(h_ref[...], w_ref[...], NN).astype(BF16)
    for s in range(2):
        v = v_all[s * BLK : (s + 1) * BLK]
        v_ref[s] = v
        cum = cum_ref[s]
        last = cum[BLK - 1 : BLK, :]
        k_dec = (k_ref[s].astype(F32) * jnp.exp(last - cum)).astype(BF16)
        delta_ref[s, 0] = dot(v, k_dec, TN).astype(BF16)


def final_kernel(
    pair,
    q_ref,
    k_ref,
    g_ref,
    bias_ref,
    cum_ref,
    do_ref,
    v_ref,
    state_ref,
    dstate_ref,
    dq_ref,
    dk_ref,
    dg_ref,
):
    row, col = iota_pair((BLK, BLK))
    row2, col2 = iota_pair((BLK, 2 * BLK))
    sums = ((col2 >= row2) & (col2 < BLK) | (col2 - BLK < row2) & (col2 >= BLK)).astype(BF16)
    for s in range(2):
        for j in range(pair):
            keys = slice(j * DK, (j + 1) * DK)
            vals = slice(j * DV, (j + 1) * DV)
            cum = cum_ref[s, :, keys]
            last = cum[BLK - 1 : BLK, :]
            q_scale = SCALE * jnp.exp(cum)
            inv_scale = jnp.exp(-cum)
            dec_scale = jnp.exp(last - cum)
            k = k_ref[s, :, keys].astype(F32)
            q_dec = (q_ref[s, :, keys].astype(F32) * q_scale).astype(BF16)
            k_inv = (k * inv_scale).astype(BF16)
            k_dec = (k * dec_scale).astype(BF16)
            do = do_ref[s, :, vals]
            v = v_ref[s, :, vals]
            state = state_ref[s, j]
            dstate = dstate_ref[s, j]
            dscores = jnp.where(row >= col, dot(do, v, NT), 0.0).astype(BF16)
            dq_intra = dot(dscores, k_inv, NN)
            dk_inv = dot(dscores, q_dec, TN)
            dq_inter = dot(do, state, NN)
            dk_dec = dot(v, dstate, NN)
            dq_ref[s, :, keys] = (q_scale * (dq_intra + dq_inter)).astype(BF16)
            dk_ref[s, :, keys] = (inv_scale * dk_inv + dec_scale * dk_dec).astype(BF16)
            q_dec = q_dec.astype(F32)
            after = q_dec * (dq_intra + dq_inter) - k_inv.astype(F32) * dk_inv
            before = k_dec.astype(F32) * dk_dec
            hi, lo = split2(jnp.concatenate([after, before], axis=0))
            through = jnp.sum(state.astype(F32) * dstate.astype(F32), axis=0, keepdims=True)
            dlog = dot(sums, hi, NN) + dot(sums, lo, NN) + jnp.exp(last) * through
            x = g_ref[s, :, keys].astype(F32) + bias_ref[:, keys]
            slope = (1.0 / SOFTNESS) / (1.0 + jnp.exp(x))
            dg_ref[s, :, keys] = (dlog * slope).astype(BF16)


def local(hidden_in, query_act, key_act, gate_act, decay_bias, value_weight, out_grad):
    positions, sequences, width = hidden_in.shape
    blocks = lax.axis_size("sp")
    weight = lax.all_gather(value_weight, "dp", axis=0, tiled=True)
    items = sequences * HEADS
    pair = 2
    steps = HEADS // pair

    q = jnp.transpose(query_act, (1, 0, 2))
    k = jnp.transpose(key_act, (1, 0, 2))
    g = jnp.transpose(gate_act, (1, 0, 2))
    do = jnp.transpose(out_grad, (1, 0, 2))
    flat = jnp.transpose(hidden_in, (1, 0, 2)).reshape(sequences * positions, width)
    bias = decay_bias.reshape(1, HEADS * DK)

    key_spec = pl.BlockSpec((2, BLK, pair * DK), lambda i: (0, 0, i))
    val_spec = pl.BlockSpec((2, BLK, pair * DV), lambda i: (0, 0, i))
    bias_spec = pl.BlockSpec((1, pair * DK), lambda i: (0, i))
    state_spec = pl.BlockSpec((2, pair, DV, DK), lambda i: (0, i, 0, 0))
    key_shape = (sequences, positions, HEADS * DK)
    val_shape = (sequences, positions, HEADS * DV)
    state_shape = (sequences, HEADS, DV, DK)
    mm = 2 * BLK * DK * DV * items

    delta, cum = pl.pallas_call(
        functools.partial(decay_kernel, pair),
        grid=(steps,),
        in_specs=[key_spec, key_spec, bias_spec, val_spec],
        out_specs=[
            pl.BlockSpec((2, pair, DV + EXTRA, DK), lambda i: (0, i, 0, 0)),
            key_spec,
        ],
        out_shape=[
            jax.ShapeDtypeStruct((sequences, HEADS, DV + EXTRA, DK), BF16),
            jax.ShapeDtypeStruct(key_shape, F32),
        ],
        compiler_params=params(),
        cost_estimate=cost(3 * mm, 5 << 20),
        name="decay",
    )(q, g, bias, do)

    rx = lax.all_to_all(
        delta.reshape(items, DV + EXTRA, DK), "sp", split_axis=0, concat_axis=0, tiled=True
    )
    dv_intra = pl.pallas_call(
        functools.partial(intra_kernel, pair),
        grid=(steps,),
        in_specs=[key_spec, key_spec, key_spec, val_spec],
        out_specs=val_spec,
        out_shape=jax.ShapeDtypeStruct(val_shape, F32),
        compiler_params=params(),
        cost_estimate=cost(3 * mm, 5 << 20),
        name="intra",
    )(q, k, cum, do)

    tails = lax.slice_in_dim(rx, DV, DV + EXTRA, axis=1)

    def scan(arrived, reverse):
        return pl.pallas_call(
            functools.partial(scan_kernel, blocks, reverse),
            out_shape=jax.ShapeDtypeStruct((blocks, DV, DK), BF16),
            cost_estimate=cost(mm, 3 << 20),
            name="scan",
        )(arrived, tails)

    dstate = lax.all_to_all(scan(rx, True), "sp", split_axis=0, concat_axis=0, tiled=True)
    dstate = dstate.reshape(state_shape)

    dv = pl.pallas_call(
        functools.partial(value_grad_kernel, pair),
        grid=(steps,),
        in_specs=[key_spec, key_spec, state_spec, val_spec],
        out_specs=val_spec,
        out_shape=jax.ShapeDtypeStruct(val_shape, BF16),
        compiler_params=params(),
        cost_estimate=cost(mm, 5 << 20),
        name="value_grad",
    )(k, cum, dstate, dv_intra)
    flat_dv = dv.reshape(sequences * positions, HEADS * DV)

    partial = dot(flat, flat_dv, TN).astype(BF16)
    partial = lax.psum_scatter(partial, "dp", scatter_dimension=0, tiled=True)

    v, vdelta = pl.pallas_call(
        project_kernel,
        grid=(HEADS,),
        in_specs=[
            pl.BlockSpec((sequences * positions, width), lambda i: (0, 0)),
            pl.BlockSpec((width, DV), lambda i: (0, i)),
            pl.BlockSpec((2, BLK, DK), lambda i: (0, 0, i)),
            pl.BlockSpec((2, BLK, DK), lambda i: (0, 0, i)),
        ],
        out_specs=[
            pl.BlockSpec((2, BLK, DV), lambda i: (0, 0, i)),
            pl.BlockSpec((2, 1, DV, DK), lambda i: (0, i, 0, 0)),
        ],
        out_shape=[
            jax.ShapeDtypeStruct(val_shape, BF16),
            jax.ShapeDtypeStruct(state_shape, BF16),
        ],
        compiler_params=params(),
        cost_estimate=cost(2 * 256 * width * HEADS * DV + mm, 12 << 20),
        name="project",
    )(flat, weight, k, cum)

    vrx = lax.all_to_all(
        vdelta.reshape(items, DV, DK), "sp", split_axis=0, concat_axis=0, tiled=True
    )
    state = lax.all_to_all(scan(vrx, False), "sp", split_axis=0, concat_axis=0, tiled=True)
    state = state.reshape(state_shape)

    hidden_grad = dot(flat_dv, weight, NT).astype(BF16)

    dq, dk, dg = pl.pallas_call(
        functools.partial(final_kernel, pair),
        grid=(steps,),
        in_specs=[
            key_spec,
            key_spec,
            key_spec,
            bias_spec,
            key_spec,
            val_spec,
            val_spec,
            state_spec,
            state_spec,
        ],
        out_specs=[key_spec, key_spec, key_spec],
        out_shape=[jax.ShapeDtypeStruct(key_shape, BF16)] * 3,
        compiler_params=params(),
        cost_estimate=cost(6 * mm, 10 << 20),
        name="final",
    )(q, k, g, bias, cum, do, v, state, dstate)

    tiles = partial.reshape(partial.shape[0], blocks, -1).transpose(1, 0, 2)
    tiles = lax.all_to_all(tiles, "sp", split_axis=0, concat_axis=0, tiled=True)
    weight_grad = jnp.sum(tiles.astype(F32), axis=0)

    def back(value):
        return jnp.transpose(value.reshape(sequences, positions, -1), (1, 0, 2))

    return (back(hidden_grad), back(dq), back(dk), back(dg), weight_grad)


def solution(mesh):
    return jax.shard_map(
        local,
        mesh=mesh,
        in_specs=(
            P("sp", "dp", None),
            P("sp", "dp", None),
            P("sp", "dp", None),
            P("sp", "dp", None),
            P(),
            P("dp", None),
            P("sp", "dp", None),
        ),
        out_specs=(
            P("sp", "dp", None),
            P("sp", "dp", None),
            P("sp", "dp", None),
            P("sp", "dp", None),
            P("dp", "sp"),
        ),
        check_vma=False,
    )
```

```python
import functools

import jax
import jax.numpy as jnp
from jax import lax
from jax.experimental import pallas as pl
from jax.experimental.pallas import tpu as pltpu
from jax.sharding import PartitionSpec as P

HEADS = 8
DK = 128
DV = 256
BLK = 128
EXTRA = 16
SOFTNESS = 16.0
SCALE = DK**-0.5
F32 = jnp.float32
BF16 = jnp.bfloat16

NN = (((1,), (0,)), ((), ()))
NT = (((1,), (1,)), ((), ()))
TN = (((0,), (0,)), ((), ()))


def dot(a, b, dims):
    return lax.dot_general(a, b, dims, preferred_element_type=F32)


def split2(x):
    hi = x.astype(BF16)
    lo = (x - hi.astype(F32)).astype(BF16)
    return hi, lo


def iota_pair(shape):
    return (
        lax.broadcasted_iota(jnp.int32, shape, 0),
        lax.broadcasted_iota(jnp.int32, shape, 1),
    )


def cost(flops, moved):
    return pl.CostEstimate(flops=flops, bytes_accessed=moved, transcendentals=0)


def params():
    return pltpu.CompilerParams(dimension_semantics=("arbitrary",))


def decay_kernel(pair, q_ref, g_ref, bias_ref, do_ref, delta_ref, cum_ref):
    row, col = iota_pair((BLK, BLK))
    lower = (row >= col).astype(BF16)
    for s in range(2):
        for j in range(pair):
            keys = slice(j * DK, (j + 1) * DK)
            x = g_ref[s, :, keys].astype(F32) + bias_ref[:, keys]
            log_decay = (jnp.minimum(x, 0.0) - jnp.log1p(jnp.exp(-jnp.abs(x)))) / SOFTNESS
            hi, lo = split2(log_decay)
            cum = dot(lower, hi, NN) + dot(lower, lo, NN)
            cum_ref[s, :, keys] = cum
            q_dec = (q_ref[s, :, keys].astype(F32) * SCALE * jnp.exp(cum)).astype(BF16)
            delta = dot(do_ref[s, :, j * DV : (j + 1) * DV], q_dec, TN)
            delta_ref[s, j, :DV, :] = delta.astype(BF16)
            last = cum[BLK - 1 : BLK, :]
            one, two = split2(last)
            three = (last - one.astype(F32) - two.astype(F32)).astype(BF16)
            rows = lax.broadcasted_iota(jnp.int32, (EXTRA, DK), 0)
            tail = jnp.where(
                rows == 0,
                one.astype(F32),
                jnp.where(rows == 1, two.astype(F32), three.astype(F32)),
            )
            delta_ref[s, j, DV:, :] = tail.astype(BF16)


def intra_kernel(pair, q_ref, k_ref, cum_ref, scores_ref, k_dec_ref):
    row, col = iota_pair((BLK, BLK))
    for s in range(2):
        for j in range(pair):
            keys = slice(j * DK, (j + 1) * DK)
            cum = cum_ref[s, :, keys]
            last = cum[BLK - 1 : BLK, :]
            k = k_ref[s, :, keys].astype(F32)
            q_dec = (q_ref[s, :, keys].astype(F32) * SCALE * jnp.exp(cum)).astype(BF16)
            k_inv = (k * jnp.exp(-cum)).astype(BF16)
            scores = dot(q_dec, k_inv, NT)
            scores_ref[s, j] = jnp.where(row >= col, scores, 0.0).astype(BF16)
            k_dec_ref[s, :, keys] = (k * jnp.exp(last - cum)).astype(BF16)


def scan_kernel(blocks, reverse, rx_ref, last_ref, out_ref):
    state = jnp.zeros(out_ref.shape[1:], F32)
    order = range(blocks - 1, -1, -1) if reverse else range(blocks)
    for b in order:
        out_ref[b] = state.astype(BF16)
        tail = last_ref[b].astype(F32)
        decay = jnp.exp(tail[0:1] + tail[1:2] + tail[2:3])
        state = state * decay + rx_ref[b].astype(F32)


def value_grad_kernel(
    pair, scores_ref, do_ref, k_dec_ref, dstate_ref, turned_ref, dv_ref, part_ref
):
    rows = []
    for s in range(2):
        heads = []
        for j in range(pair):
            vals = slice(j * DV, (j + 1) * DV)
            k_dec = k_dec_ref[s, :, j * DK : (j + 1) * DK]
            intra = dot(scores_ref[s, j], do_ref[s, :, vals], TN)
            dv = (intra + dot(k_dec, dstate_ref[s, j], NT)).astype(BF16)
            dv_ref[s, :, vals] = dv
            heads.append(dv)
        rows.append(jnp.concatenate(heads, axis=1))
    dv_all = jnp.concatenate(rows, axis=0)
    group, tiles, height, span = part_ref.shape
    for m in range(group):
        part = dot(turned_ref[m * height : (m + 1) * height, :], dv_all, NN).astype(BF16)
        for t in range(tiles):
            part_ref[m, t] = part[:, t * span : (t + 1) * span]


def project_kernel(pair, h_ref, w_ref, k_dec_ref, v_ref, delta_ref):
    v_all = dot(h_ref[...], w_ref[...], NN).astype(BF16)
    for s in range(2):
        v_ref[s] = v_all[s * BLK : (s + 1) * BLK]
        for j in range(pair):
            v = v_all[s * BLK : (s + 1) * BLK, j * DV : (j + 1) * DV]
            k_dec = k_dec_ref[s, :, j * DK : (j + 1) * DK]
            delta_ref[s, j] = dot(v, k_dec, TN).astype(BF16)


def final_kernel(
    pair,
    q_ref,
    k_ref,
    g_ref,
    bias_ref,
    cum_ref,
    do_ref,
    v_ref,
    state_ref,
    dstate_ref,
    dq_ref,
    dk_ref,
    dg_ref,
):
    row, col = iota_pair((BLK, BLK))
    row2, col2 = iota_pair((BLK, 2 * BLK))
    sums = ((col2 >= row2) & (col2 < BLK) | (col2 - BLK < row2) & (col2 >= BLK)).astype(BF16)
    for s in range(2):
        for j in range(pair):
            keys = slice(j * DK, (j + 1) * DK)
            vals = slice(j * DV, (j + 1) * DV)
            cum = cum_ref[s, :, keys]
            last = cum[BLK - 1 : BLK, :]
            q_scale = SCALE * jnp.exp(cum)
            inv_scale = jnp.exp(-cum)
            dec_scale = jnp.exp(last - cum)
            k = k_ref[s, :, keys].astype(F32)
            q_dec = (q_ref[s, :, keys].astype(F32) * q_scale).astype(BF16)
            k_inv = (k * inv_scale).astype(BF16)
            k_dec = (k * dec_scale).astype(BF16)
            do = do_ref[s, :, vals]
            v = v_ref[s, :, vals]
            state = state_ref[s, j]
            dstate = dstate_ref[s, j]
            dscores = jnp.where(row >= col, dot(do, v, NT), 0.0).astype(BF16)
            dq_intra = dot(dscores, k_inv, NN)
            dk_inv = dot(dscores, q_dec, TN)
            dq_inter = dot(do, state, NN)
            dk_dec = dot(v, dstate, NN)
            dq_ref[s, :, keys] = (q_scale * (dq_intra + dq_inter)).astype(BF16)
            dk_ref[s, :, keys] = (inv_scale * dk_inv + dec_scale * dk_dec).astype(BF16)
            q_dec = q_dec.astype(F32)
            after = q_dec * (dq_intra + dq_inter) - k_inv.astype(F32) * dk_inv
            before = k_dec.astype(F32) * dk_dec
            hi, lo = split2(jnp.concatenate([after, before], axis=0))
            through = jnp.sum(state.astype(F32) * dstate.astype(F32), axis=0, keepdims=True)
            dlog = dot(sums, hi, NN) + dot(sums, lo, NN) + jnp.exp(last) * through
            x = g_ref[s, :, keys].astype(F32) + bias_ref[:, keys]
            slope = (1.0 / SOFTNESS) / (1.0 + jnp.exp(x))
            dg_ref[s, :, keys] = (dlog * slope).astype(BF16)


def over_sp(value):
    return lax.all_to_all(value, "sp", split_axis=0, concat_axis=0, tiled=True)


def arranged(hidden_in, query_act, key_act, gate_act, decay_bias, value_weight, out_grad):
    positions, sequences, width = hidden_in.shape
    blocks = lax.axis_size("sp")
    group = lax.axis_size("dp")
    weight = lax.all_gather(value_weight, "dp", axis=0, tiled=True)
    items = sequences * HEADS
    pair = 2
    steps = HEADS // pair
    values = HEADS * DV
    rows = sequences * positions

    q = jnp.transpose(query_act, (1, 0, 2))
    g = jnp.transpose(gate_act, (1, 0, 2))
    do = jnp.transpose(out_grad, (1, 0, 2))
    bias = decay_bias.reshape(1, HEADS * DK)

    key_spec = pl.BlockSpec((2, BLK, pair * DK), lambda i: (0, 0, i))
    val_spec = pl.BlockSpec((2, BLK, pair * DV), lambda i: (0, 0, i))
    bias_spec = pl.BlockSpec((1, pair * DK), lambda i: (0, i))
    state_spec = pl.BlockSpec((2, pair, DV, DK), lambda i: (0, i, 0, 0))
    score_spec = pl.BlockSpec((2, pair, BLK, BLK), lambda i: (0, i, 0, 0))
    key_shape = (sequences, positions, HEADS * DK)
    val_shape = (sequences, positions, values)
    state_shape = (sequences, HEADS, DV, DK)
    mm = 2 * BLK * DK * DV * items
    big = 2 * rows * width * values

    delta, cum = pl.pallas_call(
        functools.partial(decay_kernel, pair),
        grid=(steps,),
        in_specs=[key_spec, key_spec, bias_spec, val_spec],
        out_specs=[
            pl.BlockSpec((2, pair, DV + EXTRA, DK), lambda i: (0, i, 0, 0)),
            key_spec,
        ],
        out_shape=[
            jax.ShapeDtypeStruct((sequences, HEADS, DV + EXTRA, DK), BF16),
            jax.ShapeDtypeStruct(key_shape, F32),
        ],
        compiler_params=params(),
        cost_estimate=cost(3 * mm, 5 << 20),
        name="decay",
    )(q, g, bias, do)

    rx = over_sp(delta.reshape(items, DV + EXTRA, DK))

    k = jnp.transpose(key_act, (1, 0, 2))
    scores, k_dec = pl.pallas_call(
        functools.partial(intra_kernel, pair),
        grid=(steps,),
        in_specs=[key_spec, key_spec, key_spec],
        out_specs=[score_spec, key_spec],
        out_shape=[
            jax.ShapeDtypeStruct((sequences, HEADS, BLK, BLK), BF16),
            jax.ShapeDtypeStruct(key_shape, BF16),
        ],
        compiler_params=params(),
        cost_estimate=cost(3 * mm, 5 << 20),
        name="intra",
    )(q, k, cum)
    turned = jnp.transpose(hidden_in, (2, 1, 0)).reshape(width, rows)
    flat = jnp.transpose(hidden_in, (1, 0, 2)).reshape(rows, width)

    cut = 4
    band = DV // cut

    def scan(arrived, reverse):
        return pl.pallas_call(
            functools.partial(scan_kernel, blocks, reverse),
            grid=(cut,),
            in_specs=[
                pl.BlockSpec((blocks, band, DK), lambda i: (0, i, 0)),
                pl.BlockSpec((blocks, EXTRA, DK), lambda i: (0, DV // EXTRA, 0)),
            ],
            out_specs=pl.BlockSpec((blocks, band, DK), lambda i: (0, i, 0)),
            out_shape=jax.ShapeDtypeStruct((blocks, DV, DK), BF16),
            compiler_params=params(),
            cost_estimate=cost(mm, 3 << 20),
            name="scan",
        )(arrived, rx)

    dstate = over_sp(scan(rx, True)).reshape(state_shape)
    dstate, flat, turned = lax.optimization_barrier((dstate, flat, turned))

    dv, partial = pl.pallas_call(
        functools.partial(value_grad_kernel, pair),
        grid=(steps,),
        in_specs=[
            score_spec,
            val_spec,
            key_spec,
            state_spec,
            pl.BlockSpec((width, rows), lambda i: (0, 0)),
        ],
        out_specs=[
            val_spec,
            pl.BlockSpec(
                (group, blocks // steps, width // group, values // blocks),
                lambda i: (0, i, 0, 0),
            ),
        ],
        out_shape=[
            jax.ShapeDtypeStruct(val_shape, BF16),
            jax.ShapeDtypeStruct((group, blocks, width // group, values // blocks), BF16),
        ],
        compiler_params=params(),
        cost_estimate=cost(big + 2 * mm, 14 << 20),
        name="value_grad",
    )(scores, do, k_dec, dstate, turned)
    flat_dv = dv.reshape(rows, values)

    partial = partial.reshape(group * blocks, width // group, values // blocks)
    partial = lax.psum_scatter(partial, "dp", scatter_dimension=0, tiled=True)

    v, vdelta = pl.pallas_call(
        functools.partial(project_kernel, pair),
        grid=(steps,),
        in_specs=[
            pl.BlockSpec((rows, width), lambda i: (0, 0)),
            pl.BlockSpec((width, pair * DV), lambda i: (0, i)),
            key_spec,
        ],
        out_specs=[val_spec, state_spec],
        out_shape=[
            jax.ShapeDtypeStruct(val_shape, BF16),
            jax.ShapeDtypeStruct(state_shape, BF16),
        ],
        compiler_params=params(),
        cost_estimate=cost(big + mm, 12 << 20),
        name="project",
    )(flat, weight, k_dec)

    vrx = over_sp(vdelta.reshape(items, DV, DK))
    state = over_sp(scan(vrx, False)).reshape(state_shape)

    hidden_grad = dot(flat_dv, weight, NT).astype(BF16)

    dq, dk, dg = pl.pallas_call(
        functools.partial(final_kernel, pair),
        grid=(steps,),
        in_specs=[
            key_spec,
            key_spec,
            key_spec,
            bias_spec,
            key_spec,
            val_spec,
            val_spec,
            state_spec,
            state_spec,
        ],
        out_specs=[key_spec, key_spec, key_spec],
        out_shape=[jax.ShapeDtypeStruct(key_shape, BF16)] * 3,
        compiler_params=params(),
        cost_estimate=cost(6 * mm, 10 << 20),
        name="final",
    )(q, k, g, bias, cum, do, v, state, dstate)

    weight_grad = jnp.sum(over_sp(partial).astype(F32), axis=0)

    def back(value):
        return jnp.transpose(value.reshape(sequences, positions, -1), (1, 0, 2))

    return (back(hidden_grad), back(dq), back(dk), back(dg), weight_grad)


def solution(mesh):
    return jax.shard_map(
        arranged,
        mesh=mesh,
        in_specs=(
            P("sp", "dp", None),
            P("sp", "dp", None),
            P("sp", "dp", None),
            P("sp", "dp", None),
            P(),
            P("dp", None),
            P("sp", "dp", None),
        ),
        out_specs=(
            P("sp", "dp", None),
            P("sp", "dp", None),
            P("sp", "dp", None),
            P("sp", "dp", None),
            P("dp", "sp"),
        ),
        check_vma=False,
    )
```

```python
import functools

import jax
import jax.numpy as jnp
from jax import lax
from jax.experimental import pallas as pl
from jax.experimental.pallas import tpu as pltpu
from jax.sharding import PartitionSpec as P

HEADS = 8
DK = 128
DV = 256
BLK = 128
SEQS = 2
ROWS = SEQS * BLK
EXTRA = 16
SOFTNESS = 16.0
SCALE = DK**-0.5
PAIR = 4
STEPS = HEADS // PAIR
F32 = jnp.float32
BF16 = jnp.bfloat16

NN = (((1,), (0,)), ((), ()))
NT = (((1,), (1,)), ((), ()))
TN = (((0,), (0,)), ((), ()))


def dot(a, b, dims):
    return lax.dot_general(a, b, dims, preferred_element_type=F32)


def split2(x):
    hi = x.astype(BF16)
    lo = (x - hi.astype(F32)).astype(BF16)
    return hi, lo


def iota_pair(shape):
    return (
        lax.broadcasted_iota(jnp.int32, shape, 0),
        lax.broadcasted_iota(jnp.int32, shape, 1),
    )


def causal():
    row, col = iota_pair((ROWS, ROWS))
    return (row >= col) & (((row - col) & 1) == 0)


def first_rows(width):
    return (lax.broadcasted_iota(jnp.int32, (ROWS, width), 0) & 1) == 0


def halves(x, first):
    zero = jnp.zeros_like(x)
    return jnp.concatenate([jnp.where(first, x, zero), jnp.where(first, zero, x)], axis=1)


def chosen(x, first):
    return jnp.where(first, x[:, :DK], x[:, DK:])


def last_of(cum, first):
    return jnp.where(first, cum[ROWS - 2 : ROWS - 1], cum[ROWS - 1 : ROWS])


def native(ref, cols):
    return ref[:, :, cols].reshape(ROWS, cols.stop - cols.start)


def head_slices(j):
    return slice(j * DK, (j + 1) * DK), slice(j * DV, (j + 1) * DV)


def cost(flops, moved):
    return pl.CostEstimate(flops=flops, bytes_accessed=moved, transcendentals=0)


def params():
    return pltpu.CompilerParams(dimension_semantics=("arbitrary",))


def decay_kernel(q_ref, g_ref, bias_ref, do_ref, delta_ref, cum_ref, q_dec_ref):
    lower = causal().astype(BF16)
    first = first_rows(DK)
    for j in range(PAIR):
        keys, vals = head_slices(j)
        x = native(g_ref, keys).astype(F32) + bias_ref[:, keys]
        log_decay = (jnp.minimum(x, 0.0) - jnp.log(1.0 + jnp.exp(-jnp.abs(x)))) / SOFTNESS
        sums = dot(lower, jnp.concatenate(split2(log_decay), axis=1), NN)
        cum = sums[:, :DK] + sums[:, DK:]
        cum_ref[:, keys] = cum
        q_dec = (native(q_ref, keys).astype(F32) * SCALE * jnp.exp(cum)).astype(BF16)
        q_dec_ref[:, keys] = q_dec
        delta = dot(native(do_ref, vals), halves(q_dec, first), TN)
        for s in range(SEQS):
            delta_ref[s, j, :DV, :] = delta[:, s * DK : (s + 1) * DK].astype(BF16)
            last = cum[ROWS - SEQS + s : ROWS - SEQS + s + 1]
            one, two = split2(last)
            three = last - one.astype(F32) - two.astype(F32)
            rows = lax.broadcasted_iota(jnp.int32, (EXTRA, DK), 0)
            tail = jnp.where(
                rows == 0, one.astype(F32), jnp.where(rows == 1, two.astype(F32), three)
            )
            delta_ref[s, j, DV:, :] = tail.astype(BF16)


def intra_kernel(k_ref, cum_ref, q_dec_ref, scores_ref, k_dec_ref):
    keep = causal()
    first = first_rows(DK)
    for j in range(PAIR):
        keys, _ = head_slices(j)
        cum = cum_ref[:, keys]
        k = native(k_ref, keys).astype(F32)
        k_inv = (k * jnp.exp(-cum)).astype(BF16)
        scores = dot(q_dec_ref[:, keys], k_inv, NT)
        scores_ref[j] = jnp.where(keep, scores, 0.0).astype(BF16)
        k_dec_ref[:, keys] = (k * jnp.exp(last_of(cum, first) - cum)).astype(BF16)


def scan_kernel(blocks, reverse, rx_ref, last_ref, out_ref):
    state = jnp.zeros((DV, DK), F32)
    order = range(blocks - 1, -1, -1) if reverse else range(blocks)
    for b in order:
        out_ref[b] = state.astype(BF16)
        tail = last_ref[b, DV:, :].astype(F32)
        decay = jnp.exp(tail[0:1] + tail[1:2] + tail[2:3])
        state = state * decay + rx_ref[b, :DV, :].astype(F32)


def value_grad_kernel(
    scores_ref, do_ref, k_dec_ref, dstate_ref, h_ref, dv_ref, part_ref
):
    first = first_rows(DK)
    heads = []
    for j in range(PAIR):
        keys, vals = head_slices(j)
        intra = dot(scores_ref[j], native(do_ref, vals), TN)
        dstate = jnp.concatenate([dstate_ref[0, j], dstate_ref[1, j]], axis=1)
        inter = dot(halves(k_dec_ref[:, keys], first), dstate, NT)
        dv = (intra + inter).astype(BF16)
        dv_ref[:, vals] = dv
        heads.append(dv)
    dv_all = jnp.concatenate(heads, axis=1)
    group, tiles, height, span = part_ref.shape
    for m in range(group):
        hidden = native(h_ref, slice(m * height, (m + 1) * height))
        part = dot(hidden, dv_all, TN).astype(BF16)
        for t in range(tiles):
            part_ref[m, t] = part[:, t * span : (t + 1) * span]


def project_kernel(h_ref, w_ref, k_dec_ref, v_ref, delta_ref):
    first = first_rows(DK)
    hidden = native(h_ref, slice(0, h_ref.shape[2]))
    v_all = dot(hidden, w_ref[...], NN).astype(BF16)
    v_ref[...] = v_all
    for j in range(PAIR):
        keys, vals = head_slices(j)
        delta = dot(v_all[:, vals], halves(k_dec_ref[:, keys], first), TN)
        for s in range(SEQS):
            delta_ref[s, j] = delta[:, s * DK : (s + 1) * DK].astype(BF16)


def hidden_grad_kernel(dv_ref, w_ref, out_ref):
    grad = dot(dv_ref[...], w_ref[...], NT).astype(BF16)
    out_ref[...] = grad.reshape(out_ref.shape)


def final_kernel(
    k_ref,
    g_ref,
    bias_ref,
    cum_ref,
    q_dec_ref,
    do_ref,
    v_ref,
    state_ref,
    dstate_ref,
    dq_ref,
    dk_ref,
    dg_ref,
):
    keep = causal()
    first = first_rows(DK)
    row, col = iota_pair((ROWS, ROWS))
    same = ((row - col) & 1) == 0
    sums = jnp.concatenate(
        [(same & (col >= row)).astype(BF16), (same & (col < row)).astype(BF16)], axis=1
    )
    for j in range(PAIR):
        keys, vals = head_slices(j)
        cum = cum_ref[:, keys]
        last = last_of(cum, first)
        q_scale = SCALE * jnp.exp(cum)
        inv_scale = jnp.exp(-cum)
        dec_scale = jnp.exp(last - cum)
        k = native(k_ref, keys).astype(F32)
        q_dec = q_dec_ref[:, keys]
        k_inv = (k * inv_scale).astype(BF16)
        k_dec = (k * dec_scale).astype(BF16)
        do = native(do_ref, vals)
        v = v_ref[:, vals]
        state = jnp.concatenate([state_ref[0, j], state_ref[1, j]], axis=1)
        dstate = jnp.concatenate([dstate_ref[0, j], dstate_ref[1, j]], axis=1)
        dscores = jnp.where(keep, dot(do, v, NT), 0.0).astype(BF16)
        dq_dec = dot(dscores, k_inv, NN) + chosen(dot(do, state, NN), first)
        dk_inv = dot(dscores, q_dec, TN)
        dk_dec = chosen(dot(v, dstate, NN), first)
        dq_ref[:, :, keys] = (q_scale * dq_dec).astype(BF16).reshape(BLK, SEQS, DK)
        dk = (inv_scale * dk_inv + dec_scale * dk_dec).astype(BF16)
        dk_ref[:, :, keys] = dk.reshape(BLK, SEQS, DK)
        after = q_dec.astype(F32) * dq_dec - k_inv.astype(F32) * dk_inv
        before = k_dec.astype(F32) * dk_dec
        terms = jnp.concatenate([after, before], axis=0)
        dlog = dot(sums, jnp.concatenate(split2(terms), axis=1), NN)
        through = jnp.sum(state.astype(F32) * dstate.astype(F32), axis=0, keepdims=True)
        through = jnp.where(first, through[:, :DK], through[:, DK:])
        dlog = dlog[:, :DK] + dlog[:, DK:] + jnp.exp(last) * through
        x = native(g_ref, keys).astype(F32) + bias_ref[:, keys]
        slope = (1.0 / SOFTNESS) / (1.0 + jnp.exp(x))
        dg_ref[:, :, keys] = (dlog * slope).astype(BF16).reshape(BLK, SEQS, DK)


def over_sp(value):
    return lax.all_to_all(value, "sp", split_axis=0, concat_axis=0, tiled=True)


def shaped(shape, dtype=BF16):
    return jax.ShapeDtypeStruct(shape, dtype)


def arranged(hidden_in, query_act, key_act, gate_act, decay_bias, value_weight, out_grad):
    _, sequences, width = hidden_in.shape
    blocks = lax.axis_size("sp")
    group = lax.axis_size("dp")
    weight = lax.all_gather(value_weight, "dp", axis=0, tiled=True)
    items = sequences * HEADS
    values = HEADS * DV
    bias = decay_bias.reshape(1, HEADS * DK)

    raw_key = pl.BlockSpec((BLK, SEQS, PAIR * DK), lambda i: (0, 0, i))
    raw_val = pl.BlockSpec((BLK, SEQS, PAIR * DV), lambda i: (0, 0, i))
    bias_spec = pl.BlockSpec((1, PAIR * DK), lambda i: (0, i))
    key_spec = pl.BlockSpec((ROWS, PAIR * DK), lambda i: (0, i))
    val_spec = pl.BlockSpec((ROWS, PAIR * DV), lambda i: (0, i))
    state_spec = pl.BlockSpec((SEQS, PAIR, DV, DK), lambda i: (0, i, 0, 0))
    score_spec = pl.BlockSpec((PAIR, ROWS, ROWS), lambda i: (i, 0, 0))
    raw_key_shape = (BLK, SEQS, HEADS * DK)
    key_shape = (ROWS, HEADS * DK)
    val_shape = (ROWS, values)
    state_shape = (SEQS, HEADS, DV, DK)
    mm = 2 * BLK * DK * DV * items
    big = 2 * ROWS * width * values

    delta, cum, q_dec = pl.pallas_call(
        decay_kernel,
        grid=(STEPS,),
        in_specs=[raw_key, raw_key, bias_spec, raw_val],
        out_specs=[
            pl.BlockSpec((SEQS, PAIR, DV + EXTRA, DK), lambda i: (0, i, 0, 0)),
            key_spec,
            key_spec,
        ],
        out_shape=[
            shaped((SEQS, HEADS, DV + EXTRA, DK)),
            shaped(key_shape, F32),
            shaped(key_shape),
        ],
        compiler_params=params(),
        cost_estimate=cost(3 * mm, 5 << 20),
        name="decay",
    )(query_act, gate_act, bias, out_grad)

    rx = over_sp(delta.reshape(items, DV + EXTRA, DK))

    scores, k_dec = pl.pallas_call(
        intra_kernel,
        grid=(STEPS,),
        in_specs=[raw_key, key_spec, key_spec],
        out_specs=[score_spec, key_spec],
        out_shape=[shaped((HEADS, ROWS, ROWS)), shaped(key_shape)],
        compiler_params=params(),
        cost_estimate=cost(3 * mm, 5 << 20),
        name="intra",
    )(key_act, cum, q_dec)

    def scan(arrived, reverse):
        return pl.pallas_call(
            functools.partial(scan_kernel, blocks, reverse),
            out_shape=shaped((blocks, DV, DK)),
            compiler_params=pltpu.CompilerParams(vmem_limit_bytes=12 << 20),
            cost_estimate=cost(mm, 3 << 20),
            name="scan",
        )(arrived, rx)

    dstate = over_sp(scan(rx, True)).reshape(state_shape)

    dv, partial = pl.pallas_call(
        value_grad_kernel,
        grid=(STEPS,),
        in_specs=[
            score_spec,
            raw_val,
            key_spec,
            state_spec,
            pl.BlockSpec((BLK, SEQS, width), lambda i: (0, 0, 0)),
        ],
        out_specs=[
            val_spec,
            pl.BlockSpec(
                (group, blocks // STEPS, width // group, values // blocks),
                lambda i: (0, i, 0, 0),
            ),
        ],
        out_shape=[
            shaped(val_shape),
            shaped((group, blocks, width // group, values // blocks)),
        ],
        compiler_params=params(),
        cost_estimate=cost(big + 2 * mm, 14 << 20),
        name="value_grad",
    )(scores, out_grad, k_dec, dstate, hidden_in)

    partial = partial.reshape(group * blocks, width // group, values // blocks)
    partial = lax.psum_scatter(partial, "dp", scatter_dimension=0, tiled=True)

    v, vdelta = pl.pallas_call(
        project_kernel,
        grid=(STEPS,),
        in_specs=[
            pl.BlockSpec((BLK, SEQS, width), lambda i: (0, 0, 0)),
            pl.BlockSpec((width, PAIR * DV), lambda i: (0, i)),
            key_spec,
        ],
        out_specs=[val_spec, state_spec],
        out_shape=[shaped(val_shape), shaped(state_shape)],
        compiler_params=params(),
        cost_estimate=cost(big + mm, 12 << 20),
        name="project",
    )(hidden_in, weight, k_dec)

    vrx = over_sp(vdelta.reshape(items, DV, DK))
    state = over_sp(scan(vrx, False)).reshape(state_shape)

    hidden_grad = pl.pallas_call(
        hidden_grad_kernel,
        grid=(4,),
        in_specs=[
            pl.BlockSpec(val_shape, lambda i: (0, 0)),
            pl.BlockSpec((width // 4, values), lambda i: (i, 0)),
        ],
        out_specs=pl.BlockSpec((BLK, SEQS, width // 4), lambda i: (0, 0, i)),
        out_shape=shaped((BLK, SEQS, width)),
        compiler_params=params(),
        cost_estimate=cost(big, 10 << 20),
        name="hidden_grad",
    )(dv, weight)

    dq, dk, dg = pl.pallas_call(
        final_kernel,
        grid=(STEPS,),
        in_specs=[
            raw_key,
            raw_key,
            bias_spec,
            key_spec,
            key_spec,
            raw_val,
            val_spec,
            state_spec,
            state_spec,
        ],
        out_specs=[raw_key, raw_key, raw_key],
        out_shape=[shaped(raw_key_shape)] * 3,
        compiler_params=params(),
        cost_estimate=cost(6 * mm, 10 << 20),
        name="final",
    )(key_act, gate_act, bias, cum, q_dec, out_grad, v, state, dstate)

    weight_grad = jnp.sum(over_sp(partial).astype(F32), axis=0)
    return (hidden_grad, dq, dk, dg, weight_grad)


def solution(mesh):
    rows = P("sp", "dp", None)
    return jax.shard_map(
        arranged,
        mesh=mesh,
        in_specs=(rows, rows, rows, rows, P(), P("dp", None), rows),
        out_specs=(rows, rows, rows, rows, P("dp", "sp")),
        check_vma=False,
    )
```

```python
import functools

import jax
import jax.numpy as jnp
from jax import lax
from jax.experimental import pallas as pl
from jax.experimental.pallas import tpu as pltpu
from jax.sharding import PartitionSpec as P

HEADS = 8
DK = 128
DV = 256
BLK = 128
SEQS = 2
ROWS = SEQS * BLK
EXTRA = 16
SOFTNESS = 16.0
SCALE = DK**-0.5
PAIR = 4
STEPS = HEADS // PAIR
F32 = jnp.float32
STRIP = 16
BF16 = jnp.bfloat16

NN = (((1,), (0,)), ((), ()))
NT = (((1,), (1,)), ((), ()))
TN = (((0,), (0,)), ((), ()))


def dot(a, b, dims):
    return lax.dot_general(a, b, dims, preferred_element_type=F32)


def split2(x):
    hi = x.astype(BF16)
    lo = (x - hi.astype(F32)).astype(BF16)
    return hi, lo


def iota_pair(shape):
    return (
        lax.broadcasted_iota(jnp.int32, shape, 0),
        lax.broadcasted_iota(jnp.int32, shape, 1),
    )


def causal():
    row, col = iota_pair((ROWS, ROWS))
    return (row >= col) & (((row - col) & 1) == 0)


def first_rows(width):
    return (lax.broadcasted_iota(jnp.int32, (ROWS, width), 0) & 1) == 0


def halves(x, first):
    zero = jnp.zeros_like(x)
    return jnp.concatenate([jnp.where(first, x, zero), jnp.where(first, zero, x)], axis=1)


def chosen(x, first):
    return jnp.where(first, x[:, :DK], x[:, DK:])


def last_of(cum, first):
    return jnp.where(first, cum[ROWS - 2 : ROWS - 1], cum[ROWS - 1 : ROWS])


def native(ref, cols):
    if cols.stop - cols.start == DK:
        parts = [
            ref[i : i + STRIP, :, cols].reshape(SEQS * STRIP, DK)
            for i in range(0, BLK, STRIP)
        ]
        return jnp.concatenate(parts, axis=0)
    return ref[:, :, cols].reshape(ROWS, cols.stop - cols.start)


def put(ref, cols, x):
    for i in range(0, BLK, STRIP):
        part = x[SEQS * i : SEQS * (i + STRIP)]
        ref[i : i + STRIP, :, cols] = part.reshape(STRIP, SEQS, DK)


def head_slices(j):
    return slice(j * DK, (j + 1) * DK), slice(j * DV, (j + 1) * DV)


def cost(flops, moved):
    return pl.CostEstimate(flops=flops, bytes_accessed=moved, transcendentals=0)


def params():
    return pltpu.CompilerParams(dimension_semantics=("arbitrary",))


def decay_kernel(q_ref, g_ref, bias_ref, do_ref, delta_ref, cum_ref, q_dec_ref):
    lower = causal().astype(BF16)
    first = first_rows(DK)
    for j in range(PAIR):
        keys, vals = head_slices(j)
        x = native(g_ref, keys).astype(F32) + bias_ref[:, keys]
        log_decay = (jnp.minimum(x, 0.0) - jnp.log(1.0 + jnp.exp(-jnp.abs(x)))) / SOFTNESS
        sums = dot(lower, jnp.concatenate(split2(log_decay), axis=1), NN)
        cum = sums[:, :DK] + sums[:, DK:]
        cum_ref[:, keys] = cum
        q_dec = (native(q_ref, keys).astype(F32) * SCALE * jnp.exp(cum)).astype(BF16)
        q_dec_ref[:, keys] = q_dec
        delta = dot(native(do_ref, vals), halves(q_dec, first), TN)
        for s in range(SEQS):
            delta_ref[s, j, :DV, :] = delta[:, s * DK : (s + 1) * DK].astype(BF16)
            last = cum[ROWS - SEQS + s : ROWS - SEQS + s + 1]
            one, two = split2(last)
            three = last - one.astype(F32) - two.astype(F32)
            rows = lax.broadcasted_iota(jnp.int32, (EXTRA, DK), 0)
            tail = jnp.where(
                rows == 0, one.astype(F32), jnp.where(rows == 1, two.astype(F32), three)
            )
            delta_ref[s, j, DV:, :] = tail.astype(BF16)


def intra_kernel(k_ref, cum_ref, q_dec_ref, scores_ref, k_dec_ref):
    keep = causal()
    first = first_rows(DK)
    for j in range(PAIR):
        keys, _ = head_slices(j)
        cum = cum_ref[:, keys]
        k = native(k_ref, keys).astype(F32)
        k_inv = (k * jnp.exp(-cum)).astype(BF16)
        scores = dot(q_dec_ref[:, keys], k_inv, NT)
        scores_ref[j] = jnp.where(keep, scores, 0.0).astype(BF16)
        k_dec_ref[:, keys] = (k * jnp.exp(last_of(cum, first) - cum)).astype(BF16)


def scan_kernel(blocks, reverse, rx_ref, last_ref, out_ref):
    state = jnp.zeros((DV, DK), F32)
    order = range(blocks - 1, -1, -1) if reverse else range(blocks)
    for b in order:
        out_ref[b] = state.astype(BF16)
        tail = last_ref[b, DV:, :].astype(F32)
        decay = jnp.exp(tail[0:1] + tail[1:2] + tail[2:3])
        state = state * decay + rx_ref[b, :DV, :].astype(F32)


def value_grad_kernel(
    scores_ref, do_ref, k_dec_ref, dstate_ref, h_ref, dv_ref, part_ref
):
    first = first_rows(DK)
    heads = []
    for j in range(PAIR):
        keys, vals = head_slices(j)
        intra = dot(scores_ref[j], native(do_ref, vals), TN)
        dstate = jnp.concatenate([dstate_ref[0, j], dstate_ref[1, j]], axis=1)
        inter = dot(halves(k_dec_ref[:, keys], first), dstate, NT)
        dv = (intra + inter).astype(BF16)
        dv_ref[:, vals] = dv
        heads.append(dv)
    dv_all = jnp.concatenate(heads, axis=1)
    group, tiles, height, span = part_ref.shape
    for m in range(group):
        hidden = native(h_ref, slice(m * height, (m + 1) * height))
        part = dot(hidden, dv_all, TN).astype(BF16)
        for t in range(tiles):
            part_ref[m, t] = part[:, t * span : (t + 1) * span]


def project_kernel(h_ref, w_ref, k_dec_ref, v_ref, delta_ref):
    first = first_rows(DK)
    hidden = native(h_ref, slice(0, h_ref.shape[2]))
    v_all = dot(hidden, w_ref[...], NN).astype(BF16)
    v_ref[...] = v_all
    for j in range(PAIR):
        keys, vals = head_slices(j)
        delta = dot(v_all[:, vals], halves(k_dec_ref[:, keys], first), TN)
        for s in range(SEQS):
            delta_ref[s, j] = delta[:, s * DK : (s + 1) * DK].astype(BF16)


def hidden_grad_kernel(dv_ref, w_ref, out_ref):
    grad = dot(dv_ref[...], w_ref[...], NT).astype(BF16)
    out_ref[...] = grad.reshape(out_ref.shape)


def final_kernel(
    k_ref,
    g_ref,
    bias_ref,
    cum_ref,
    q_dec_ref,
    do_ref,
    v_ref,
    state_ref,
    dstate_ref,
    dq_ref,
    dk_ref,
    dg_ref,
):
    keep = causal()
    first = first_rows(DK)
    row, col = iota_pair((ROWS, ROWS))
    same = ((row - col) & 1) == 0
    sums = jnp.concatenate(
        [(same & (col >= row)).astype(BF16), (same & (col < row)).astype(BF16)], axis=1
    )
    for j in range(PAIR):
        keys, vals = head_slices(j)
        cum = cum_ref[:, keys]
        last = last_of(cum, first)
        q_scale = SCALE * jnp.exp(cum)
        inv_scale = jnp.exp(-cum)
        dec_scale = jnp.exp(last - cum)
        k = native(k_ref, keys).astype(F32)
        q_dec = q_dec_ref[:, keys]
        k_inv = (k * inv_scale).astype(BF16)
        k_dec = (k * dec_scale).astype(BF16)
        do = native(do_ref, vals)
        v = v_ref[:, vals]
        state = jnp.concatenate([state_ref[0, j], state_ref[1, j]], axis=1)
        dstate = jnp.concatenate([dstate_ref[0, j], dstate_ref[1, j]], axis=1)
        dscores = jnp.where(keep, dot(do, v, NT), 0.0).astype(BF16)
        dq_dec = dot(dscores, k_inv, NN) + chosen(dot(do, state, NN), first)
        dk_inv = dot(dscores, q_dec, TN)
        dk_dec = chosen(dot(v, dstate, NN), first)
        put(dq_ref, keys, (q_scale * dq_dec).astype(BF16))
        dk = (inv_scale * dk_inv + dec_scale * dk_dec).astype(BF16)
        put(dk_ref, keys, dk)
        after = q_dec.astype(F32) * dq_dec - k_inv.astype(F32) * dk_inv
        before = k_dec.astype(F32) * dk_dec
        terms = jnp.concatenate([after, before], axis=0)
        dlog = dot(sums, jnp.concatenate(split2(terms), axis=1), NN)
        through = jnp.sum(state.astype(F32) * dstate.astype(F32), axis=0, keepdims=True)
        through = jnp.where(first, through[:, :DK], through[:, DK:])
        dlog = dlog[:, :DK] + dlog[:, DK:] + jnp.exp(last) * through
        x = native(g_ref, keys).astype(F32) + bias_ref[:, keys]
        slope = (1.0 / SOFTNESS) / (1.0 + jnp.exp(x))
        put(dg_ref, keys, (dlog * slope).astype(BF16))


def over_sp(value):
    return lax.all_to_all(value, "sp", split_axis=0, concat_axis=0, tiled=True)


def shaped(shape, dtype=BF16):
    return jax.ShapeDtypeStruct(shape, dtype)


def arranged(hidden_in, query_act, key_act, gate_act, decay_bias, value_weight, out_grad):
    _, sequences, width = hidden_in.shape
    blocks = lax.axis_size("sp")
    group = lax.axis_size("dp")
    weight = lax.all_gather(value_weight, "dp", axis=0, tiled=True)
    items = sequences * HEADS
    values = HEADS * DV
    bias = decay_bias.reshape(1, HEADS * DK)

    raw_key = pl.BlockSpec((BLK, SEQS, PAIR * DK), lambda i: (0, 0, i))
    raw_val = pl.BlockSpec((BLK, SEQS, PAIR * DV), lambda i: (0, 0, i))
    bias_spec = pl.BlockSpec((1, PAIR * DK), lambda i: (0, i))
    key_spec = pl.BlockSpec((ROWS, PAIR * DK), lambda i: (0, i))
    val_spec = pl.BlockSpec((ROWS, PAIR * DV), lambda i: (0, i))
    state_spec = pl.BlockSpec((SEQS, PAIR, DV, DK), lambda i: (0, i, 0, 0))
    score_spec = pl.BlockSpec((PAIR, ROWS, ROWS), lambda i: (i, 0, 0))
    raw_key_shape = (BLK, SEQS, HEADS * DK)
    key_shape = (ROWS, HEADS * DK)
    val_shape = (ROWS, values)
    state_shape = (SEQS, HEADS, DV, DK)
    mm = 2 * BLK * DK * DV * items
    big = 2 * ROWS * width * values

    delta, cum, q_dec = pl.pallas_call(
        decay_kernel,
        grid=(STEPS,),
        in_specs=[raw_key, raw_key, bias_spec, raw_val],
        out_specs=[
            pl.BlockSpec((SEQS, PAIR, DV + EXTRA, DK), lambda i: (0, i, 0, 0)),
            key_spec,
            key_spec,
        ],
        out_shape=[
            shaped((SEQS, HEADS, DV + EXTRA, DK)),
            shaped(key_shape, F32),
            shaped(key_shape),
        ],
        compiler_params=params(),
        cost_estimate=cost(3 * mm, 5 << 20),
        name="decay",
    )(query_act, gate_act, bias, out_grad)

    rx = over_sp(delta.reshape(items, DV + EXTRA, DK))

    scores, k_dec = pl.pallas_call(
        intra_kernel,
        grid=(STEPS,),
        in_specs=[raw_key, key_spec, key_spec],
        out_specs=[score_spec, key_spec],
        out_shape=[shaped((HEADS, ROWS, ROWS)), shaped(key_shape)],
        compiler_params=params(),
        cost_estimate=cost(3 * mm, 5 << 20),
        name="intra",
    )(key_act, cum, q_dec)

    def scan(arrived, reverse):
        return pl.pallas_call(
            functools.partial(scan_kernel, blocks, reverse),
            out_shape=shaped((blocks, DV, DK)),
            compiler_params=pltpu.CompilerParams(vmem_limit_bytes=12 << 20),
            cost_estimate=cost(mm, 3 << 20),
            name="scan",
        )(arrived, rx)

    dstate = over_sp(scan(rx, True)).reshape(state_shape)

    dv, partial = pl.pallas_call(
        value_grad_kernel,
        grid=(STEPS,),
        in_specs=[
            score_spec,
            raw_val,
            key_spec,
            state_spec,
            pl.BlockSpec((BLK, SEQS, width), lambda i: (0, 0, 0)),
        ],
        out_specs=[
            val_spec,
            pl.BlockSpec(
                (group, blocks // STEPS, width // group, values // blocks),
                lambda i: (0, i, 0, 0),
            ),
        ],
        out_shape=[
            shaped(val_shape),
            shaped((group, blocks, width // group, values // blocks)),
        ],
        compiler_params=params(),
        cost_estimate=cost(big + 2 * mm, 14 << 20),
        name="value_grad",
    )(scores, out_grad, k_dec, dstate, hidden_in)

    partial = partial.reshape(group * blocks, width // group, values // blocks)
    partial = lax.psum_scatter(partial, "dp", scatter_dimension=0, tiled=True)

    v, vdelta = pl.pallas_call(
        project_kernel,
        grid=(STEPS,),
        in_specs=[
            pl.BlockSpec((BLK, SEQS, width), lambda i: (0, 0, 0)),
            pl.BlockSpec((width, PAIR * DV), lambda i: (0, i)),
            key_spec,
        ],
        out_specs=[val_spec, state_spec],
        out_shape=[shaped(val_shape), shaped(state_shape)],
        compiler_params=params(),
        cost_estimate=cost(big + mm, 12 << 20),
        name="project",
    )(hidden_in, weight, k_dec)

    vrx = over_sp(vdelta.reshape(items, DV, DK))
    state = over_sp(scan(vrx, False)).reshape(state_shape)

    hidden_grad = pl.pallas_call(
        hidden_grad_kernel,
        grid=(4,),
        in_specs=[
            pl.BlockSpec(val_shape, lambda i: (0, 0)),
            pl.BlockSpec((width // 4, values), lambda i: (i, 0)),
        ],
        out_specs=pl.BlockSpec((BLK, SEQS, width // 4), lambda i: (0, 0, i)),
        out_shape=shaped((BLK, SEQS, width)),
        compiler_params=params(),
        cost_estimate=cost(big, 10 << 20),
        name="hidden_grad",
    )(dv, weight)

    dq, dk, dg = pl.pallas_call(
        final_kernel,
        grid=(STEPS,),
        in_specs=[
            raw_key,
            raw_key,
            bias_spec,
            key_spec,
            key_spec,
            raw_val,
            val_spec,
            state_spec,
            state_spec,
        ],
        out_specs=[raw_key, raw_key, raw_key],
        out_shape=[shaped(raw_key_shape)] * 3,
        compiler_params=params(),
        cost_estimate=cost(6 * mm, 10 << 20),
        name="final",
    )(key_act, gate_act, bias, cum, q_dec, out_grad, v, state, dstate)

    weight_grad = jnp.sum(over_sp(partial).astype(F32), axis=0)
    return (hidden_grad, dq, dk, dg, weight_grad)


def solution(mesh):
    rows = P("sp", "dp", None)
    return jax.shard_map(
        arranged,
        mesh=mesh,
        in_specs=(rows, rows, rows, rows, P(), P("dp", None), rows),
        out_specs=(rows, rows, rows, rows, P("dp", "sp")),
        check_vma=False,
    )
```

```python
import functools

import jax
import jax.numpy as jnp
from jax import lax
from jax.experimental import pallas as pl
from jax.experimental.pallas import tpu as pltpu
from jax.sharding import PartitionSpec as P

HEADS = 8
DK = 128
DV = 256
BLK = 128
SEQS = 2
ROWS = SEQS * BLK
EXTRA = 8
SOFTNESS = 16.0
SCALE = DK**-0.5
PAIR = 4
STEPS = HEADS // PAIR
F32 = jnp.float32
STRIP = 16
BF16 = jnp.bfloat16

NN = (((1,), (0,)), ((), ()))
NT = (((1,), (1,)), ((), ()))
TN = (((0,), (0,)), ((), ()))


def dot(a, b, dims):
    return lax.dot_general(a, b, dims, preferred_element_type=F32)


def split2(x):
    hi = x.astype(BF16)
    lo = (x - hi.astype(F32)).astype(BF16)
    return hi, lo


def iota_pair(shape):
    return (
        lax.broadcasted_iota(jnp.int32, shape, 0),
        lax.broadcasted_iota(jnp.int32, shape, 1),
    )


def causal():
    row, col = iota_pair((ROWS, ROWS))
    return (row >= col) & (((row - col) & 1) == 0)


def first_rows(width):
    return (lax.broadcasted_iota(jnp.int32, (ROWS, width), 0) & 1) == 0


def halves(x, first):
    zero = jnp.zeros_like(x)
    return jnp.concatenate([jnp.where(first, x, zero), jnp.where(first, zero, x)], axis=1)


def chosen(x, first):
    return jnp.where(first, x[:, :DK], x[:, DK:])


def last_of(cum, first):
    return jnp.where(first, cum[ROWS - 2 : ROWS - 1], cum[ROWS - 1 : ROWS])


def native(ref, cols):
    if cols.stop - cols.start == DK:
        parts = [
            ref[i : i + STRIP, :, cols].reshape(SEQS * STRIP, DK)
            for i in range(0, BLK, STRIP)
        ]
        return jnp.concatenate(parts, axis=0)
    return ref[:, :, cols].reshape(ROWS, cols.stop - cols.start)


def put(ref, cols, x):
    for i in range(0, BLK, STRIP):
        part = x[SEQS * i : SEQS * (i + STRIP)]
        ref[i : i + STRIP, :, cols] = part.reshape(STRIP, SEQS, DK)


def head_slices(j):
    return slice(j * DK, (j + 1) * DK), slice(j * DV, (j + 1) * DV)


def cost(flops, moved):
    return pl.CostEstimate(flops=flops, bytes_accessed=moved, transcendentals=0)


def params():
    return pltpu.CompilerParams(dimension_semantics=("arbitrary",))


def decayed(q_ref, g_ref, bias_ref, keys, lower):
    x = native(g_ref, keys).astype(F32) + bias_ref[:, keys]
    log_decay = (jnp.minimum(x, 0.0) - jnp.log(1.0 + jnp.exp(-jnp.abs(x)))) / SOFTNESS
    sums = dot(lower, jnp.concatenate(split2(log_decay), axis=1), NN)
    cum = sums[:, :DK] + sums[:, DK:]
    q_dec = (native(q_ref, keys).astype(F32) * SCALE * jnp.exp(cum)).astype(BF16)
    return cum, q_dec


def decay_kernel(q_ref, g_ref, bias_ref, do_ref, delta_ref):
    lower = causal().astype(BF16)
    first = first_rows(DK)
    for j in range(PAIR):
        keys, vals = head_slices(j)
        cum, q_dec = decayed(q_ref, g_ref, bias_ref, keys, lower)
        delta = dot(native(do_ref, vals), halves(q_dec, first), TN)
        for s in range(SEQS):
            delta_ref[s, j, :DV, :] = delta[:, s * DK : (s + 1) * DK].astype(BF16)
            last = cum[ROWS - SEQS + s : ROWS - SEQS + s + 1]
            one, two = split2(last)
            three = last - one.astype(F32) - two.astype(F32)
            rows = lax.broadcasted_iota(jnp.int32, (EXTRA, DK), 0)
            tail = jnp.where(
                rows == 0, one.astype(F32), jnp.where(rows == 1, two.astype(F32), three)
            )
            delta_ref[s, j, DV:, :] = tail.astype(BF16)


def intra_kernel(
    q_ref, k_ref, g_ref, bias_ref, cum_ref, q_dec_ref, scores_ref, k_dec_ref
):
    keep = causal()
    lower = keep.astype(BF16)
    first = first_rows(DK)
    for j in range(PAIR):
        keys, _ = head_slices(j)
        cum, q_dec = decayed(q_ref, g_ref, bias_ref, keys, lower)
        cum_ref[:, keys] = cum
        q_dec_ref[:, keys] = q_dec
        k = native(k_ref, keys).astype(F32)
        k_inv = (k * jnp.exp(-cum)).astype(BF16)
        scores = dot(q_dec, k_inv, NT)
        scores_ref[j] = jnp.where(keep, scores, 0.0).astype(BF16)
        k_dec_ref[:, keys] = (k * jnp.exp(last_of(cum, first) - cum)).astype(BF16)


def scan_kernel(blocks, reverse, rx_ref, last_ref, out_ref):
    state = jnp.zeros((DV, DK), F32)
    order = range(blocks - 1, -1, -1) if reverse else range(blocks)
    for b in order:
        out_ref[b] = state.astype(BF16)
        tail = last_ref[b, DV:, :].astype(F32)
        decay = jnp.exp(tail[0:1] + tail[1:2] + tail[2:3])
        state = state * decay + rx_ref[b, :DV, :].astype(F32)


def value_grad_kernel(scores_ref, do_ref, k_dec_ref, dstate_ref, dv_ref):
    first = first_rows(DK)
    for j in range(PAIR):
        keys, vals = head_slices(j)
        intra = dot(scores_ref[j], native(do_ref, vals), TN)
        dstate = jnp.concatenate([dstate_ref[0, j], dstate_ref[1, j]], axis=1)
        inter = dot(halves(k_dec_ref[:, keys], first), dstate, NT)
        dv_ref[:, vals] = (intra + inter).astype(BF16)


def pick_kernel(order_ref, h_ref, out_ref):
    out_ref[...] = h_ref[...]


def part_kernel(order_ref, h_ref, got_ref, dv_ref, dv_got_ref, top_ref, bottom_ref):
    cols = slice(0, h_ref.shape[2])
    part = dot(native(h_ref, cols), dv_ref[...], TN)
    part = (part + dot(native(got_ref, cols), dv_got_ref[...], TN)).astype(BF16)
    half = part.shape[0] // 2
    top_ref[...] = part[:half]
    bottom_ref[...] = part[half:]


def rest_kernel(order_ref, h_ref, got_ref, dv_ref, dv_got_ref, *outs):
    cols = slice(0, h_ref.shape[2])
    part = dot(native(h_ref, cols), dv_ref[...], TN)
    part = (part + dot(native(got_ref, cols), dv_got_ref[...], TN)).astype(BF16)
    half = part.shape[0] // 2
    for p in range(3):

        @pl.when(pl.program_id(0) == p)
        def _():
            outs[2 * p][...] = part[:half]
            outs[2 * p + 1][...] = part[half:]


def join_kernel(top_refs, bottom_refs, out_ref):
    tiles, _, span = out_ref.shape
    half = top_refs[0].shape[0]
    for refs, start in ((top_refs, 0), (bottom_refs, half)):
        total = refs[0][...].astype(F32) + refs[1][...].astype(F32)
        total = (total + refs[2][...].astype(F32)).astype(BF16)
        for t in range(tiles):
            out_ref[t, start : start + half] = total[:, t * span : (t + 1) * span]


def join_parts(*refs):
    join_kernel(refs[:3], refs[3:6], refs[6])


def project_kernel(
    order_ref, h_ref, near_ref, near_got_ref, far_ref, far_got_ref, k_dec_ref,
    v_ref, delta_ref, held,
):
    first = first_rows(DK)
    shard = far_ref.shape[0]

    @pl.when(pl.program_id(0) == 0)
    def _():
        for p in range(held.shape[1] // shard):
            start = pl.multiple_of(order_ref[p] * shard, shard)
            cols = h_ref[:, :, pl.ds(start, shard)].reshape(ROWS, shard)
            held[:, p * shard : (p + 1) * shard] = cols

    v_all = jnp.zeros(v_ref.shape, F32)
    start = 0
    for ref in (near_ref, near_got_ref, far_ref, far_got_ref):
        v_all += dot(held[:, start : start + ref.shape[0]], ref[...], NN)
        start += ref.shape[0]
    v_all = v_all.astype(BF16)
    v_ref[...] = v_all
    for j in range(PAIR):
        keys, vals = head_slices(j)
        delta = dot(v_all[:, vals], halves(k_dec_ref[:, keys], first), TN)
        for s in range(SEQS):
            delta_ref[s, j] = delta[:, s * DK : (s + 1) * DK].astype(BF16)


def hidden_grad_kernel(
    order_ref, dv_ref, near_ref, near_got_ref, far_ref, far_got_ref, out_ref
):
    p = pl.program_id(0)

    def emit(ref):
        grad = dot(dv_ref[...], ref[...], NT).astype(BF16)
        out_ref[...] = grad.reshape(out_ref.shape)

    pl.when(p < 3)(lambda: emit(near_ref))
    pl.when((p >= 3) & (p < 6))(lambda: emit(near_got_ref))
    pl.when(p == 6)(lambda: emit(far_ref))
    pl.when(p == 7)(lambda: emit(far_got_ref))


def final_kernel(
    k_ref,
    g_ref,
    bias_ref,
    cum_ref,
    q_dec_ref,
    do_ref,
    v_ref,
    state_ref,
    dstate_ref,
    dq_ref,
    dk_ref,
    dg_ref,
):
    keep = causal()
    first = first_rows(DK)
    row, col = iota_pair((ROWS, ROWS))
    same = ((row - col) & 1) == 0
    sums = jnp.concatenate(
        [(same & (col >= row)).astype(BF16), (same & (col < row)).astype(BF16)], axis=1
    )
    for j in range(PAIR):
        keys, vals = head_slices(j)
        cum = cum_ref[:, keys]
        last = last_of(cum, first)
        q_scale = SCALE * jnp.exp(cum)
        inv_scale = jnp.exp(-cum)
        dec_scale = jnp.exp(last - cum)
        k = native(k_ref, keys).astype(F32)
        q_dec = q_dec_ref[:, keys]
        k_inv = (k * inv_scale).astype(BF16)
        k_dec = (k * dec_scale).astype(BF16)
        do = native(do_ref, vals)
        v = v_ref[:, vals]
        state = jnp.concatenate([state_ref[0, j], state_ref[1, j]], axis=1)
        dstate = jnp.concatenate([dstate_ref[0, j], dstate_ref[1, j]], axis=1)
        dscores = jnp.where(keep, dot(do, v, NT), 0.0).astype(BF16)
        dq_dec = dot(dscores, k_inv, NN) + chosen(dot(do, state, NN), first)
        dk_inv = dot(dscores, q_dec, TN)
        dk_dec = chosen(dot(v, dstate, NN), first)
        put(dq_ref, keys, (q_scale * dq_dec).astype(BF16))
        dk = (inv_scale * dk_inv + dec_scale * dk_dec).astype(BF16)
        put(dk_ref, keys, dk)
        after = q_dec.astype(F32) * dq_dec - k_inv.astype(F32) * dk_inv
        before = k_dec.astype(F32) * dk_dec
        terms = jnp.concatenate([after, before], axis=0)
        dlog = dot(sums, jnp.concatenate(split2(terms), axis=1), NN)
        through = jnp.sum(state.astype(F32) * dstate.astype(F32), axis=0, keepdims=True)
        through = jnp.where(first, through[:, :DK], through[:, DK:])
        dlog = dlog[:, :DK] + dlog[:, DK:] + jnp.exp(last) * through
        x = native(g_ref, keys).astype(F32) + bias_ref[:, keys]
        slope = (1.0 / SOFTNESS) / (1.0 + jnp.exp(x))
        put(dg_ref, keys, (dlog * slope).astype(BF16))


def over_sp(value):
    return lax.all_to_all(value, "sp", split_axis=0, concat_axis=0, tiled=True)


def shaped(shape, dtype=BF16):
    return jax.ShapeDtypeStruct(shape, dtype)


def arranged(hidden_in, query_act, key_act, gate_act, decay_bias, value_weight, out_grad):
    _, sequences, width = hidden_in.shape
    blocks = lax.axis_size("sp")
    group = lax.axis_size("dp")
    place = lax.axis_index("dp")
    chip, core = place // 2, place % 2
    chips = group // 2
    shard = width // group
    shift = jnp.array([0, -1, 1, 0, -1, 1, 2, 2, 2, 1, -1, 0, 2, 1, -1, 0], jnp.int32)
    other = jnp.array([0, 0, 0, 1, 1, 1, 0, 1, 0, 0, 0, 0, 0, 0, 0, 0], jnp.int32)
    twice = jnp.array([2] * 12 + [1] * 4, jnp.int32)
    order = twice * ((chip + shift + chips) % chips) + (twice - 1) * ((core + other) % 2)
    order = order.astype(jnp.int32)

    def along(value, step):
        pairs = [(d, (d + 2 * step) % group) for d in range(group)]
        return lax.ppermute(value, "dp", pairs)

    def swap(value):
        return lax.ppermute(value, "dp", [(d, d ^ 1) for d in range(group)])

    half = shard // 2
    before = along(value_weight, 1)
    after = along(value_weight, -1)
    far_one = along(before[:half], 1)
    far_two = along(after[half:], -1)
    far = jnp.concatenate([far_one, far_two], axis=0)
    near = jnp.concatenate([value_weight, before, after], axis=0)
    near_got = swap(near)
    far_got = swap(far)
    items = sequences * HEADS
    values = HEADS * DV
    bias = decay_bias.reshape(1, HEADS * DK)

    raw_key = pl.BlockSpec((BLK, SEQS, PAIR * DK), lambda i: (0, 0, i))
    raw_val = pl.BlockSpec((BLK, SEQS, PAIR * DV), lambda i: (0, 0, i))
    bias_spec = pl.BlockSpec((1, PAIR * DK), lambda i: (0, i))
    key_spec = pl.BlockSpec((ROWS, PAIR * DK), lambda i: (0, i))
    val_spec = pl.BlockSpec((ROWS, PAIR * DV), lambda i: (0, i))
    state_spec = pl.BlockSpec((SEQS, PAIR, DV, DK), lambda i: (0, i, 0, 0))
    score_spec = pl.BlockSpec((PAIR, ROWS, ROWS), lambda i: (i, 0, 0))
    raw_key_shape = (BLK, SEQS, HEADS * DK)
    key_shape = (ROWS, HEADS * DK)
    val_shape = (ROWS, values)
    state_shape = (SEQS, HEADS, DV, DK)
    mm = 2 * BLK * DK * DV * items
    big = 2 * ROWS * width * values

    delta = pl.pallas_call(
        decay_kernel,
        grid=(STEPS,),
        in_specs=[raw_key, raw_key, bias_spec, raw_val],
        out_specs=pl.BlockSpec((SEQS, PAIR, DV + EXTRA, DK), lambda i: (0, i, 0, 0)),
        out_shape=shaped((SEQS, HEADS, DV + EXTRA, DK)),
        compiler_params=params(),
        cost_estimate=cost(3 * mm, 4 << 20),
        name="decay",
    )(query_act, gate_act, bias, out_grad)

    rx = over_sp(delta.reshape(items, DV + EXTRA, DK))

    cum, q_dec, scores, k_dec = pl.pallas_call(
        intra_kernel,
        grid=(STEPS,),
        in_specs=[raw_key, raw_key, raw_key, bias_spec],
        out_specs=[key_spec, key_spec, score_spec, key_spec],
        out_shape=[
            shaped(key_shape, F32),
            shaped(key_shape),
            shaped((HEADS, ROWS, ROWS)),
            shaped(key_shape),
        ],
        compiler_params=params(),
        cost_estimate=cost(3 * mm, 5 << 20),
        name="intra",
    )(query_act, key_act, gate_act, bias)

    raw = (BLK, SEQS, shard)
    given = pl.pallas_call(
        pick_kernel,
        grid_spec=pltpu.PrefetchScalarGridSpec(
            num_scalar_prefetch=1,
            grid=(chips,),
            in_specs=[pl.BlockSpec(raw, lambda i, o: (0, 0, 2 * i + o[3] % 2))],
            out_specs=pl.BlockSpec(raw, lambda i, o: (0, 0, i)),
        ),
        out_shape=shaped((BLK, SEQS, width // 2)),
        compiler_params=params(),
        cost_estimate=cost(1 << 22, 1 << 20),
        name="pick",
    )(order, hidden_in)
    got = swap(given)

    def scan(arrived, reverse):
        return pl.pallas_call(
            functools.partial(scan_kernel, blocks, reverse),
            out_shape=shaped((blocks, DV, DK)),
            compiler_params=pltpu.CompilerParams(vmem_limit_bytes=12 << 20),
            cost_estimate=cost(mm, 3 << 20),
            name="scan",
        )(arrived, rx)

    dcarried = scan(rx, True)
    dstate = over_sp(dcarried).reshape(state_shape)

    dv = pl.pallas_call(
        value_grad_kernel,
        grid=(STEPS,),
        in_specs=[score_spec, raw_val, key_spec, state_spec],
        out_specs=val_spec,
        out_shape=shaped(val_shape),
        compiler_params=params(),
        cost_estimate=cost(3 * mm, 5 << 20),
        name="value_grad",
    )(scores, out_grad, k_dec, dstate)

    dv_got = swap(dv)
    turns = 2

    def part():
        raw = (BLK, SEQS, shard)
        return pl.pallas_call(
            part_kernel,
            grid_spec=pltpu.PrefetchScalarGridSpec(
                num_scalar_prefetch=1,
                grid=(turns,),
                in_specs=[
                    pl.BlockSpec(raw, lambda i, o: (0, 0, o[8])),
                    pl.BlockSpec(raw, lambda i, o: (0, 0, o[12])),
                    pl.BlockSpec((ROWS, values // turns), lambda i, o: (0, i)),
                    pl.BlockSpec((ROWS, values // turns), lambda i, o: (0, i)),
                ],
                out_specs=[pl.BlockSpec((half, values // turns), lambda i, o: (0, i))] * 2,
            ),
            out_shape=[shaped((half, values))] * 2,
            compiler_params=params(),
            cost_estimate=cost(big // 4, 5 << 20),
        )(order, hidden_in, got, dv, dv_got)

    def rest():
        raw = (BLK, SEQS, shard)
        whole = pl.BlockSpec((ROWS, values), lambda i, o: (0, 0))
        return pl.pallas_call(
            rest_kernel,
            grid_spec=pltpu.PrefetchScalarGridSpec(
                num_scalar_prefetch=1,
                grid=(3,),
                in_specs=[
                    pl.BlockSpec(raw, lambda i, o: (0, 0, o[9 + i])),
                    pl.BlockSpec(raw, lambda i, o: (0, 0, o[13 + i])),
                    whole,
                    whole,
                ],
                out_specs=[pl.BlockSpec((half, values), lambda i, o: (0, 0))] * 6,
            ),
            out_shape=[shaped((half, values))] * 6,
            compiler_params=params(),
            cost_estimate=cost(3 * big // 4, 8 << 20),
            name="part_rest",
        )(order, hidden_in, got, dv, dv_got)

    far_top, far_bottom = part()
    from_before = along(far_top, 1)
    from_after = along(far_bottom, -1)
    next_top, next_bottom, last_top, last_bottom, own_top, own_bottom = rest()
    ready_before = along(next_bottom, 1)
    ready_after = along(last_top, -1)

    def plus(one, two):
        return (one.astype(F32) + two.astype(F32)).astype(BF16)

    late_before = along(plus(next_top, from_before), 1)
    late_after = along(plus(last_bottom, from_after), -1)
    partial = pl.pallas_call(
        join_parts,
        out_shape=shaped((blocks, shard, values // blocks)),
        compiler_params=pltpu.CompilerParams(vmem_limit_bytes=20 << 20),
        cost_estimate=cost(1 << 22, 4 << 20),
        name="join",
    )(own_top, late_before, ready_after, own_bottom, ready_before, late_after)

    v, vdelta = pl.pallas_call(
        project_kernel,
        grid_spec=pltpu.PrefetchScalarGridSpec(
            num_scalar_prefetch=1,
            grid=(STEPS,),
            in_specs=[
                pl.BlockSpec((BLK, SEQS, width), lambda i, o: (0, 0, 0)),
                pl.BlockSpec((3 * shard, PAIR * DV), lambda i, o: (0, i)),
                pl.BlockSpec((3 * shard, PAIR * DV), lambda i, o: (0, i)),
                pl.BlockSpec((shard, PAIR * DV), lambda i, o: (0, i)),
                pl.BlockSpec((shard, PAIR * DV), lambda i, o: (0, i)),
                pl.BlockSpec((ROWS, PAIR * DK), lambda i, o: (0, i)),
            ],
            out_specs=[
                pl.BlockSpec((ROWS, PAIR * DV), lambda i, o: (0, i)),
                pl.BlockSpec((SEQS, PAIR, DV, DK), lambda i, o: (0, i, 0, 0)),
            ],
            scratch_shapes=[pltpu.VMEM((ROWS, width), BF16)],
        ),
        out_shape=[shaped(val_shape), shaped(state_shape)],
        compiler_params=params(),
        cost_estimate=cost(big + mm, 12 << 20),
        name="project",
    )(order, hidden_in, near, near_got, far, far_got, k_dec)

    vrx = over_sp(vdelta.reshape(items, DV, DK))
    state = over_sp(scan(vrx, False)).reshape(state_shape)

    block = (shard, values)
    hidden_grad = pl.pallas_call(
        hidden_grad_kernel,
        grid_spec=pltpu.PrefetchScalarGridSpec(
            num_scalar_prefetch=1,
            grid=(group,),
            in_specs=[
                pl.BlockSpec(val_shape, lambda i, o: (0, 0)),
                pl.BlockSpec(block, lambda i, o: (jnp.minimum(i, 2), 0)),
                pl.BlockSpec(block, lambda i, o: (jnp.clip(i - 3, 0, 2), 0)),
                pl.BlockSpec(block, lambda i, o: (0, 0)),
                pl.BlockSpec(block, lambda i, o: (0, 0)),
            ],
            out_specs=pl.BlockSpec((BLK, SEQS, shard), lambda i, o: (0, 0, o[i])),
        ),
        out_shape=shaped((BLK, SEQS, width)),
        compiler_params=params(),
        cost_estimate=cost(big, 10 << 20),
        name="hidden_grad",
    )(order, dv, near, near_got, far, far_got)

    dq, dk, dg = pl.pallas_call(
        final_kernel,
        grid=(STEPS,),
        in_specs=[
            raw_key,
            raw_key,
            bias_spec,
            key_spec,
            key_spec,
            raw_val,
            val_spec,
            state_spec,
            state_spec,
        ],
        out_specs=[raw_key, raw_key, raw_key],
        out_shape=[shaped(raw_key_shape)] * 3,
        compiler_params=params(),
        cost_estimate=cost(6 * mm, 10 << 20),
        name="final",
    )(key_act, gate_act, bias, cum, q_dec, out_grad, v, state, dstate)

    weight_grad = jnp.sum(over_sp(partial).astype(F32), axis=0)
    return (hidden_grad, dq, dk, dg, weight_grad)


def solution(mesh):
    rows = P("sp", "dp", None)
    return jax.shard_map(
        arranged,
        mesh=mesh,
        in_specs=(rows, rows, rows, rows, P(), P("dp", None), rows),
        out_specs=(rows, rows, rows, rows, P("dp", "sp")),
        check_vma=False,
    )
```

```python
import functools

import jax
import jax.numpy as jnp
from jax import lax
from jax.experimental import pallas as pl
from jax.experimental.pallas import tpu as pltpu
from jax.sharding import PartitionSpec as P

HEADS = 8
DK = 128
DV = 256
BLK = 128
SEQS = 2
ROWS = SEQS * BLK
EXTRA = 8
SOFTNESS = 16.0
SCALE = DK**-0.5
PAIR = 4
STEPS = HEADS // PAIR
F32 = jnp.float32
STRIP = 16
BF16 = jnp.bfloat16

NN = (((1,), (0,)), ((), ()))
NT = (((1,), (1,)), ((), ()))
TN = (((0,), (0,)), ((), ()))


def dot(a, b, dims):
    return lax.dot_general(a, b, dims, preferred_element_type=F32)


def split2(x):
    hi = x.astype(BF16)
    lo = (x - hi.astype(F32)).astype(BF16)
    return hi, lo


def iota_pair(shape):
    return (
        lax.broadcasted_iota(jnp.int32, shape, 0),
        lax.broadcasted_iota(jnp.int32, shape, 1),
    )


def causal():
    row, col = iota_pair((ROWS, ROWS))
    return (row >= col) & (((row - col) & 1) == 0)


def first_rows(width):
    return (lax.broadcasted_iota(jnp.int32, (ROWS, width), 0) & 1) == 0


def halves(x, first):
    zero = jnp.zeros_like(x)
    return jnp.concatenate([jnp.where(first, x, zero), jnp.where(first, zero, x)], axis=1)


def chosen(x, first):
    return jnp.where(first, x[:, :DK], x[:, DK:])


def last_of(cum, first):
    return jnp.where(first, cum[ROWS - 2 : ROWS - 1], cum[ROWS - 1 : ROWS])


def native(ref, cols):
    if cols.stop - cols.start == DK:
        parts = [
            ref[i : i + STRIP, :, cols].reshape(SEQS * STRIP, DK)
            for i in range(0, BLK, STRIP)
        ]
        return jnp.concatenate(parts, axis=0)
    return ref[:, :, cols].reshape(ROWS, cols.stop - cols.start)


def put(ref, cols, x):
    for i in range(0, BLK, STRIP):
        part = x[SEQS * i : SEQS * (i + STRIP)]
        ref[i : i + STRIP, :, cols] = part.reshape(STRIP, SEQS, DK)


def head_slices(j):
    return slice(j * DK, (j + 1) * DK), slice(j * DV, (j + 1) * DV)


def cost(flops, moved):
    return pl.CostEstimate(flops=flops, bytes_accessed=moved, transcendentals=0)


def params():
    return pltpu.CompilerParams(dimension_semantics=("arbitrary",))


def decayed(q_ref, g_ref, bias_ref, keys, lower):
    x = native(g_ref, keys).astype(F32) + bias_ref[:, keys]
    log_decay = (jnp.minimum(x, 0.0) - jnp.log(1.0 + jnp.exp(-jnp.abs(x)))) / SOFTNESS
    sums = dot(lower, jnp.concatenate(split2(log_decay), axis=1), NN)
    cum = sums[:, :DK] + sums[:, DK:]
    q_dec = (native(q_ref, keys).astype(F32) * SCALE * jnp.exp(cum)).astype(BF16)
    return cum, q_dec


def decay_kernel(q_ref, g_ref, bias_ref, do_ref, delta_ref):
    lower = causal().astype(BF16)
    first = first_rows(DK)
    for j in range(PAIR):
        keys, vals = head_slices(j)
        cum, q_dec = decayed(q_ref, g_ref, bias_ref, keys, lower)
        delta = dot(native(do_ref, vals), halves(q_dec, first), TN)
        for s in range(SEQS):
            delta_ref[s, j, :DV, :] = delta[:, s * DK : (s + 1) * DK].astype(BF16)
            last = cum[ROWS - SEQS + s : ROWS - SEQS + s + 1]
            one, two = split2(last)
            three = last - one.astype(F32) - two.astype(F32)
            rows = lax.broadcasted_iota(jnp.int32, (EXTRA, DK), 0)
            tail = jnp.where(
                rows == 0, one.astype(F32), jnp.where(rows == 1, two.astype(F32), three)
            )
            delta_ref[s, j, DV:, :] = tail.astype(BF16)


def intra_kernel(
    q_ref, k_ref, g_ref, bias_ref, cum_ref, q_dec_ref, scores_ref, k_dec_ref
):
    keep = causal()
    lower = keep.astype(BF16)
    first = first_rows(DK)
    for j in range(PAIR):
        keys, _ = head_slices(j)
        cum, q_dec = decayed(q_ref, g_ref, bias_ref, keys, lower)
        cum_ref[:, keys] = cum
        q_dec_ref[:, keys] = q_dec
        k = native(k_ref, keys).astype(F32)
        k_inv = (k * jnp.exp(-cum)).astype(BF16)
        scores = dot(q_dec, k_inv, NT)
        scores_ref[j] = jnp.where(keep, scores, 0.0).astype(BF16)
        k_dec_ref[:, keys] = (k * jnp.exp(last_of(cum, first) - cum)).astype(BF16)


def scan_kernel(blocks, reverse, rx_ref, last_ref, out_ref):
    state = jnp.zeros((DV, DK), F32)
    order = range(blocks - 1, -1, -1) if reverse else range(blocks)
    for b in order:
        out_ref[b] = state.astype(BF16)
        tail = last_ref[b, DV:, :].astype(F32)
        decay = jnp.exp(tail[0:1] + tail[1:2] + tail[2:3])
        state = state * decay + rx_ref[b, :DV, :].astype(F32)


def value_grad_kernel(scores_ref, do_ref, k_dec_ref, dstate_ref, dv_ref):
    first = first_rows(DK)
    for j in range(PAIR):
        keys, vals = head_slices(j)
        intra = dot(scores_ref[j], native(do_ref, vals), TN)
        dstate = jnp.concatenate([dstate_ref[0, j], dstate_ref[1, j]], axis=1)
        inter = dot(halves(k_dec_ref[:, keys], first), dstate, NT)
        dv_ref[:, vals] = (intra + inter).astype(BF16)


def part_kernel(order_ref, h_ref, got_ref, dv_ref, dv_got_ref, top_ref, bottom_ref):
    cols = slice(0, h_ref.shape[2])
    part = dot(native(h_ref, cols), dv_ref[...], TN)
    part = (part + dot(native(got_ref, cols), dv_got_ref[...], TN)).astype(BF16)
    half = part.shape[0] // 2
    top_ref[...] = part[:half]
    bottom_ref[...] = part[half:]


def rest_kernel(order_ref, h_ref, got_ref, dv_ref, dv_got_ref, *outs):
    cols = slice(0, h_ref.shape[2])
    part = dot(native(h_ref, cols), dv_ref[...], TN)
    part = (part + dot(native(got_ref, cols), dv_got_ref[...], TN)).astype(BF16)
    half = part.shape[0] // 2
    for p in range(3):

        @pl.when(pl.program_id(0) == p)
        def _():
            outs[2 * p][...] = part[:half]
            outs[2 * p + 1][...] = part[half:]


def join_kernel(top_refs, bottom_refs, out_ref):
    tiles, _, span = out_ref.shape
    half = top_refs[0].shape[0]
    for refs, start in ((top_refs, 0), (bottom_refs, half)):
        total = refs[0][...].astype(F32) + refs[1][...].astype(F32)
        total = (total + refs[2][...].astype(F32)).astype(BF16)
        for t in range(tiles):
            out_ref[t, start : start + half] = total[:, t * span : (t + 1) * span]


def join_parts(*refs):
    join_kernel(refs[:3], refs[3:6], refs[6])


def hold(order_ref, h_ref, held, base):
    shard = h_ref.shape[2] // 8

    @pl.when(pl.program_id(0) == 0)
    def _():
        for p in range(held.shape[1] // shard):
            start = pl.multiple_of(order_ref[base + p] * shard, shard)
            cols = h_ref[:, :, pl.ds(start, shard)].reshape(ROWS, shard)
            held[:, p * shard : (p + 1) * shard] = cols


def near_kernel(order_ref, h_ref, *refs):
    *pieces, sum_ref, held = refs
    hold(order_ref, h_ref, held, 0)
    weight = jnp.concatenate([ref[...] for ref in pieces], axis=0)
    sum_ref[...] = dot(held[...], weight, NN)


def project_kernel(order_ref, h_ref, sum_ref, k_dec_ref, *refs):
    *pieces, v_ref, delta_ref, held = refs
    first = first_rows(DK)
    hold(order_ref, h_ref, held, 6)
    weight = jnp.concatenate([ref[...] for ref in pieces], axis=0)
    v_all = (sum_ref[...] + dot(held[...], weight, NN)).astype(BF16)
    v_ref[...] = v_all
    for j in range(PAIR):
        keys, vals = head_slices(j)
        delta = dot(v_all[:, vals], halves(k_dec_ref[:, keys], first), TN)
        for s in range(SEQS):
            delta_ref[s, j] = delta[:, s * DK : (s + 1) * DK].astype(BF16)


def hidden_grad_kernel(order_ref, dv_ref, *refs):
    *pieces, out_ref = refs
    shard = out_ref.shape[2] // 2
    core = order_ref[0] % 2

    def emit(side, weight):
        grad = dot(dv_ref[...], weight, NT).astype(BF16)
        start = pl.multiple_of(side * shard, shard)
        out_ref[:, :, pl.ds(start, shard)] = grad.reshape(BLK, SEQS, shard)

    groups = (
        ((0,), (5,)),
        ((1, 2), (6, 7)),
        ((3, 4), (8, 9)),
        ((10, 11), (12, 13)),
    )
    for k, (mine, got) in enumerate(groups):

        @pl.when(pl.program_id(0) == k)
        def _():
            emit(core, jnp.concatenate([pieces[n][...] for n in mine], axis=0))
            emit(1 - core, jnp.concatenate([pieces[n][...] for n in got], axis=0))


def final_kernel(
    k_ref,
    g_ref,
    bias_ref,
    cum_ref,
    q_dec_ref,
    do_ref,
    v_ref,
    state_ref,
    dstate_ref,
    dq_ref,
    dk_ref,
    dg_ref,
):
    keep = causal()
    first = first_rows(DK)
    row, col = iota_pair((ROWS, ROWS))
    same = ((row - col) & 1) == 0
    sums = jnp.concatenate(
        [(same & (col >= row)).astype(BF16), (same & (col < row)).astype(BF16)], axis=1
    )
    for j in range(PAIR):
        keys, vals = head_slices(j)
        cum = cum_ref[:, keys]
        last = last_of(cum, first)
        q_scale = SCALE * jnp.exp(cum)
        inv_scale = jnp.exp(-cum)
        dec_scale = jnp.exp(last - cum)
        k = native(k_ref, keys).astype(F32)
        q_dec = q_dec_ref[:, keys]
        k_inv = (k * inv_scale).astype(BF16)
        k_dec = (k * dec_scale).astype(BF16)
        do = native(do_ref, vals)
        v = v_ref[:, vals]
        state = jnp.concatenate([state_ref[0, j], state_ref[1, j]], axis=1)
        dstate = jnp.concatenate([dstate_ref[0, j], dstate_ref[1, j]], axis=1)
        dscores = jnp.where(keep, dot(do, v, NT), 0.0).astype(BF16)
        dq_dec = dot(dscores, k_inv, NN) + chosen(dot(do, state, NN), first)
        dk_inv = dot(dscores, q_dec, TN)
        dk_dec = chosen(dot(v, dstate, NN), first)
        put(dq_ref, keys, (q_scale * dq_dec).astype(BF16))
        dk = (inv_scale * dk_inv + dec_scale * dk_dec).astype(BF16)
        put(dk_ref, keys, dk)
        after = q_dec.astype(F32) * dq_dec - k_inv.astype(F32) * dk_inv
        before = k_dec.astype(F32) * dk_dec
        terms = jnp.concatenate([after, before], axis=0)
        dlog = dot(sums, jnp.concatenate(split2(terms), axis=1), NN)
        through = jnp.sum(state.astype(F32) * dstate.astype(F32), axis=0, keepdims=True)
        through = jnp.where(first, through[:, :DK], through[:, DK:])
        dlog = dlog[:, :DK] + dlog[:, DK:] + jnp.exp(last) * through
        x = native(g_ref, keys).astype(F32) + bias_ref[:, keys]
        slope = (1.0 / SOFTNESS) / (1.0 + jnp.exp(x))
        put(dg_ref, keys, (dlog * slope).astype(BF16))


def over_sp(value):
    return lax.all_to_all(value, "sp", split_axis=0, concat_axis=0, tiled=True)


def shaped(shape, dtype=BF16):
    return jax.ShapeDtypeStruct(shape, dtype)


def arranged(hidden_in, query_act, key_act, gate_act, decay_bias, value_weight, out_grad):
    _, sequences, width = hidden_in.shape
    blocks = lax.axis_size("sp")
    group = lax.axis_size("dp")
    place = lax.axis_index("dp")
    chip, core = place // 2, place % 2
    chips = group // 2
    shard = width // group
    shift = jnp.array([0, -1, 1, 0, -1, 1, 2, 2, 2, 1, -1, 0, 2, 1, -1, 0], jnp.int32)
    other = jnp.array([0, 0, 0, 1, 1, 1, 0, 1, 0, 0, 0, 0, 0, 0, 0, 0], jnp.int32)
    twice = jnp.array([2] * 12 + [1] * 4, jnp.int32)
    order = twice * ((chip + shift + chips) % chips) + (twice - 1) * ((core + other) % 2)
    order = order.astype(jnp.int32)

    def along(value, step):
        pairs = [(d, (d + 2 * step) % group) for d in range(group)]
        return lax.ppermute(value, "dp", pairs)

    def swap(value):
        return lax.ppermute(value, "dp", [(d, d ^ 1) for d in range(group)])

    half = shard // 2
    top, bottom = value_weight[:half], value_weight[half:]

    before_top = along(top, 1)
    after_bottom = along(bottom, -1)
    before_bottom = along(bottom, 1)
    after_top = along(top, -1)
    far_one = along(before_top, 1)
    far_two = along(after_bottom, -1)

    near = [value_weight, before_top, before_bottom, after_top, after_bottom]
    near += [swap(value) for value in near]
    far = [far_one, far_two]
    far += [swap(far_one), swap(far_two)]
    items = sequences * HEADS
    values = HEADS * DV
    bias = decay_bias.reshape(1, HEADS * DK)

    raw_key = pl.BlockSpec((BLK, SEQS, PAIR * DK), lambda i: (0, 0, i))
    raw_val = pl.BlockSpec((BLK, SEQS, PAIR * DV), lambda i: (0, 0, i))
    bias_spec = pl.BlockSpec((1, PAIR * DK), lambda i: (0, i))
    key_spec = pl.BlockSpec((ROWS, PAIR * DK), lambda i: (0, i))
    val_spec = pl.BlockSpec((ROWS, PAIR * DV), lambda i: (0, i))
    state_spec = pl.BlockSpec((SEQS, PAIR, DV, DK), lambda i: (0, i, 0, 0))
    score_spec = pl.BlockSpec((PAIR, ROWS, ROWS), lambda i: (i, 0, 0))
    raw_key_shape = (BLK, SEQS, HEADS * DK)
    key_shape = (ROWS, HEADS * DK)
    val_shape = (ROWS, values)
    state_shape = (SEQS, HEADS, DV, DK)
    mm = 2 * BLK * DK * DV * items
    big = 2 * ROWS * width * values

    delta = pl.pallas_call(
        decay_kernel,
        grid=(STEPS,),
        in_specs=[raw_key, raw_key, bias_spec, raw_val],
        out_specs=pl.BlockSpec((SEQS, PAIR, DV + EXTRA, DK), lambda i: (0, i, 0, 0)),
        out_shape=shaped((SEQS, HEADS, DV + EXTRA, DK)),
        compiler_params=params(),
        cost_estimate=cost(3 * mm, 4 << 20),
        name="decay",
    )(query_act, gate_act, bias, out_grad)

    rx = over_sp(delta.reshape(items, DV + EXTRA, DK))

    cum, q_dec, scores, k_dec = pl.pallas_call(
        intra_kernel,
        grid=(STEPS,),
        in_specs=[raw_key, raw_key, raw_key, bias_spec],
        out_specs=[key_spec, key_spec, score_spec, key_spec],
        out_shape=[
            shaped(key_shape, F32),
            shaped(key_shape),
            shaped((HEADS, ROWS, ROWS)),
            shaped(key_shape),
        ],
        compiler_params=params(),
        cost_estimate=cost(3 * mm, 5 << 20),
        name="intra",
    )(query_act, key_act, gate_act, bias)

    got = swap(hidden_in)

    def scan(arrived, reverse):
        return pl.pallas_call(
            functools.partial(scan_kernel, blocks, reverse),
            out_shape=shaped((blocks, DV, DK)),
            compiler_params=pltpu.CompilerParams(vmem_limit_bytes=12 << 20),
            cost_estimate=cost(mm, 3 << 20),
            name="scan",
        )(arrived, rx)

    dcarried = scan(rx, True)
    dstate = over_sp(dcarried).reshape(state_shape)

    dv = pl.pallas_call(
        value_grad_kernel,
        grid=(STEPS,),
        in_specs=[score_spec, raw_val, key_spec, state_spec],
        out_specs=val_spec,
        out_shape=shaped(val_shape),
        compiler_params=params(),
        cost_estimate=cost(3 * mm, 5 << 20),
        name="value_grad",
    )(scores, out_grad, k_dec, dstate)

    dv_got = swap(dv)
    turns = 2

    def part():
        raw = (BLK, SEQS, shard)
        return pl.pallas_call(
            part_kernel,
            grid_spec=pltpu.PrefetchScalarGridSpec(
                num_scalar_prefetch=1,
                grid=(turns,),
                in_specs=[
                    pl.BlockSpec(raw, lambda i, o: (0, 0, o[8])),
                    pl.BlockSpec(raw, lambda i, o: (0, 0, o[8])),
                    pl.BlockSpec((ROWS, values // turns), lambda i, o: (0, i)),
                    pl.BlockSpec((ROWS, values // turns), lambda i, o: (0, i)),
                ],
                out_specs=[pl.BlockSpec((half, values // turns), lambda i, o: (0, i))] * 2,
            ),
            out_shape=[shaped((half, values))] * 2,
            compiler_params=params(),
            cost_estimate=cost(big // 4, 5 << 20),
        )(order, hidden_in, got, dv, dv_got)

    def rest():
        raw = (BLK, SEQS, shard)
        whole = pl.BlockSpec((ROWS, values), lambda i, o: (0, 0))
        return pl.pallas_call(
            rest_kernel,
            grid_spec=pltpu.PrefetchScalarGridSpec(
                num_scalar_prefetch=1,
                grid=(3,),
                in_specs=[
                    pl.BlockSpec(raw, lambda i, o: (0, 0, o[9 + i])),
                    pl.BlockSpec(raw, lambda i, o: (0, 0, o[9 + i])),
                    whole,
                    whole,
                ],
                out_specs=[pl.BlockSpec((half, values), lambda i, o: (0, 0))] * 6,
            ),
            out_shape=[shaped((half, values))] * 6,
            compiler_params=params(),
            cost_estimate=cost(3 * big // 4, 8 << 20),
            name="part_rest",
        )(order, hidden_in, got, dv, dv_got)

    far_top, far_bottom = part()
    from_before = along(far_top, 1)
    from_after = along(far_bottom, -1)
    next_top, next_bottom, last_top, last_bottom, own_top, own_bottom = rest()
    ready_before = along(next_bottom, 1)
    ready_after = along(last_top, -1)

    def plus(one, two):
        return (one.astype(F32) + two.astype(F32)).astype(BF16)

    late_before = along(plus(next_top, from_before), 1)
    late_after = along(plus(last_bottom, from_after), -1)
    partial = pl.pallas_call(
        join_parts,
        out_shape=shaped((blocks, shard, values // blocks)),
        compiler_params=pltpu.CompilerParams(vmem_limit_bytes=20 << 20),
        cost_estimate=cost(1 << 22, 4 << 20),
        name="join",
    )(own_top, late_before, ready_after, own_bottom, ready_before, late_after)

    hidden_spec = pl.BlockSpec((BLK, SEQS, width), lambda i, o: (0, 0, 0))
    wide = pl.BlockSpec((ROWS, PAIR * DV), lambda i, o: (0, i))
    near_spec = pl.BlockSpec((shard, PAIR * DV), lambda i, o: (0, i))
    far_spec = pl.BlockSpec((half, PAIR * DV), lambda i, o: (0, i))
    near_sum = pl.pallas_call(
        near_kernel,
        grid_spec=pltpu.PrefetchScalarGridSpec(
            num_scalar_prefetch=1,
            grid=(STEPS,),
            in_specs=[hidden_spec] + ([near_spec] + [far_spec] * 4) * 2,
            out_specs=wide,
            scratch_shapes=[pltpu.VMEM((ROWS, 6 * shard), BF16)],
        ),
        out_shape=shaped(val_shape, F32),
        compiler_params=params(),
        cost_estimate=cost(3 * big // 4, 10 << 20),
        name="project_near",
    )(order, hidden_in, *near)

    v, vdelta = pl.pallas_call(
        project_kernel,
        grid_spec=pltpu.PrefetchScalarGridSpec(
            num_scalar_prefetch=1,
            grid=(STEPS,),
            in_specs=[
                hidden_spec,
                wide,
                pl.BlockSpec((ROWS, PAIR * DK), lambda i, o: (0, i)),
            ]
            + [far_spec] * 4,
            out_specs=[
                wide,
                pl.BlockSpec((SEQS, PAIR, DV, DK), lambda i, o: (0, i, 0, 0)),
            ],
            scratch_shapes=[pltpu.VMEM((ROWS, 2 * shard), BF16)],
        ),
        out_shape=[shaped(val_shape), shaped(state_shape)],
        compiler_params=params(),
        cost_estimate=cost(big // 4 + mm, 7 << 20),
        name="project",
    )(order, hidden_in, near_sum, k_dec, *far)

    vrx = over_sp(vdelta.reshape(items, DV, DK))
    state = over_sp(scan(vrx, False)).reshape(state_shape)

    whole = pl.BlockSpec((shard, values), lambda i, o: (0, 0))
    part_whole = pl.BlockSpec((half, values), lambda i, o: (0, 0))
    hidden_grad = pl.pallas_call(
        hidden_grad_kernel,
        grid_spec=pltpu.PrefetchScalarGridSpec(
            num_scalar_prefetch=1,
            grid=(chips,),
            in_specs=[pl.BlockSpec(val_shape, lambda i, o: (0, 0))]
            + ([whole] + [part_whole] * 4) * 2
            + [part_whole] * 4,
            out_specs=pl.BlockSpec((BLK, SEQS, 2 * shard), lambda i, o: (0, 0, o[15 - i])),
        ),
        out_shape=shaped((BLK, SEQS, width)),
        compiler_params=params(),
        cost_estimate=cost(big, 10 << 20),
        name="hidden_grad",
    )(order, dv, *near, *far)

    dq, dk, dg = pl.pallas_call(
        final_kernel,
        grid=(STEPS,),
        in_specs=[
            raw_key,
            raw_key,
            bias_spec,
            key_spec,
            key_spec,
            raw_val,
            val_spec,
            state_spec,
            state_spec,
        ],
        out_specs=[raw_key, raw_key, raw_key],
        out_shape=[shaped(raw_key_shape)] * 3,
        compiler_params=params(),
        cost_estimate=cost(6 * mm, 10 << 20),
        name="final",
    )(key_act, gate_act, bias, cum, q_dec, out_grad, v, state, dstate)

    weight_grad = jnp.sum(over_sp(partial).astype(F32), axis=0)
    return (hidden_grad, dq, dk, dg, weight_grad)


def solution(mesh):
    rows = P("sp", "dp", None)
    return jax.shard_map(
        arranged,
        mesh=mesh,
        in_specs=(rows, rows, rows, rows, P(), P("dp", None), rows),
        out_specs=(rows, rows, rows, rows, P("dp", "sp")),
        check_vma=False,
    )
```

```python
import functools

import jax
import jax.numpy as jnp
from jax import lax
from jax.experimental import pallas as pl
from jax.experimental.pallas import tpu as pltpu
from jax.sharding import PartitionSpec as P

HEADS = 8
DK = 128
DV = 256
BLK = 128
SEQS = 2
ROWS = SEQS * BLK
EXTRA = 8
SOFTNESS = 16.0
SCALE = DK**-0.5
PAIR = 4
STEPS = HEADS // PAIR
F32 = jnp.float32
STRIP = 16
BF16 = jnp.bfloat16

NN = (((1,), (0,)), ((), ()))
NT = (((1,), (1,)), ((), ()))
TN = (((0,), (0,)), ((), ()))


def dot(a, b, dims):
    return lax.dot_general(a, b, dims, preferred_element_type=F32)


def split2(x):
    hi = x.astype(BF16)
    lo = (x - hi.astype(F32)).astype(BF16)
    return hi, lo


def iota_pair(shape):
    return (
        lax.broadcasted_iota(jnp.int32, shape, 0),
        lax.broadcasted_iota(jnp.int32, shape, 1),
    )


def causal():
    row, col = iota_pair((ROWS, ROWS))
    return (row >= col) & (((row - col) & 1) == 0)


def first_rows(width):
    return (lax.broadcasted_iota(jnp.int32, (ROWS, width), 0) & 1) == 0


def halves(x, first):
    zero = jnp.zeros_like(x)
    return jnp.concatenate([jnp.where(first, x, zero), jnp.where(first, zero, x)], axis=1)


def chosen(x, first):
    return jnp.where(first, x[:, :DK], x[:, DK:])


def last_of(cum, first):
    return jnp.where(first, cum[ROWS - 2 : ROWS - 1], cum[ROWS - 1 : ROWS])


def native(ref, cols):
    if cols.stop - cols.start == DK:
        parts = [
            ref[i : i + STRIP, :, cols].reshape(SEQS * STRIP, DK)
            for i in range(0, BLK, STRIP)
        ]
        return jnp.concatenate(parts, axis=0)
    return ref[:, :, cols].reshape(ROWS, cols.stop - cols.start)


def put(ref, cols, x):
    for i in range(0, BLK, STRIP):
        part = x[SEQS * i : SEQS * (i + STRIP)]
        ref[i : i + STRIP, :, cols] = part.reshape(STRIP, SEQS, DK)


def head_slices(j):
    return slice(j * DK, (j + 1) * DK), slice(j * DV, (j + 1) * DV)


def cost(flops, moved):
    return pl.CostEstimate(flops=flops, bytes_accessed=moved, transcendentals=0)


def params():
    return pltpu.CompilerParams(dimension_semantics=("arbitrary",))


def decayed(q_ref, g_ref, bias_ref, keys, lower):
    x = native(g_ref, keys).astype(F32) + bias_ref[:, keys]
    log_decay = (jnp.minimum(x, 0.0) - jnp.log(1.0 + jnp.exp(-jnp.abs(x)))) / SOFTNESS
    sums = dot(lower, jnp.concatenate(split2(log_decay), axis=1), NN)
    cum = sums[:, :DK] + sums[:, DK:]
    q_dec = (native(q_ref, keys).astype(F32) * SCALE * jnp.exp(cum)).astype(BF16)
    return cum, q_dec


def decay_kernel(q_ref, g_ref, bias_ref, do_ref, delta_ref):
    lower = causal().astype(BF16)
    first = first_rows(DK)
    for j in range(PAIR):
        keys, vals = head_slices(j)
        cum, q_dec = decayed(q_ref, g_ref, bias_ref, keys, lower)
        delta = dot(native(do_ref, vals), halves(q_dec, first), TN)
        for s in range(SEQS):
            delta_ref[s, j, :DV, :] = delta[:, s * DK : (s + 1) * DK].astype(BF16)
            last = cum[ROWS - SEQS + s : ROWS - SEQS + s + 1]
            one, two = split2(last)
            three = last - one.astype(F32) - two.astype(F32)
            rows = lax.broadcasted_iota(jnp.int32, (EXTRA, DK), 0)
            tail = jnp.where(
                rows == 0, one.astype(F32), jnp.where(rows == 1, two.astype(F32), three)
            )
            delta_ref[s, j, DV:, :] = tail.astype(BF16)


def intra_kernel(
    q_ref, k_ref, g_ref, bias_ref, cum_ref, q_dec_ref, scores_ref, k_dec_ref
):
    keep = causal()
    lower = keep.astype(BF16)
    first = first_rows(DK)
    for j in range(PAIR):
        keys, _ = head_slices(j)
        cum, q_dec = decayed(q_ref, g_ref, bias_ref, keys, lower)
        cum_ref[:, keys] = cum
        q_dec_ref[:, keys] = q_dec
        k = native(k_ref, keys).astype(F32)
        k_inv = (k * jnp.exp(-cum)).astype(BF16)
        scores = dot(q_dec, k_inv, NT)
        scores_ref[j] = jnp.where(keep, scores, 0.0).astype(BF16)
        k_dec_ref[:, keys] = (k * jnp.exp(last_of(cum, first) - cum)).astype(BF16)


def scan_kernel(blocks, reverse, rx_ref, last_ref, out_ref):
    state = jnp.zeros((DV, DK), F32)
    order = range(blocks - 1, -1, -1) if reverse else range(blocks)
    for b in order:
        out_ref[b] = state.astype(BF16)
        tail = last_ref[b, DV:, :].astype(F32)
        decay = jnp.exp(tail[0:1] + tail[1:2] + tail[2:3])
        state = state * decay + rx_ref[b, :DV, :].astype(F32)


def value_grad_kernel(scores_ref, do_ref, k_dec_ref, dstate_ref, dv_ref):
    first = first_rows(DK)
    for j in range(PAIR):
        keys, vals = head_slices(j)
        intra = dot(scores_ref[j], native(do_ref, vals), TN)
        dstate = jnp.concatenate([dstate_ref[0, j], dstate_ref[1, j]], axis=1)
        inter = dot(halves(k_dec_ref[:, keys], first), dstate, NT)
        dv_ref[:, vals] = (intra + inter).astype(BF16)


def part_kernel(order_ref, h_ref, got_ref, dv_ref, dv_got_ref, top_ref, bottom_ref):
    cols = slice(0, h_ref.shape[2])
    part = dot(native(h_ref, cols), dv_ref[...], TN)
    part = (part + dot(native(got_ref, cols), dv_got_ref[...], TN)).astype(BF16)
    half = part.shape[0] // 2
    top_ref[...] = part[:half]
    bottom_ref[...] = part[half:]


def rest_kernel(order_ref, h_ref, got_ref, dv_ref, dv_got_ref, *outs):
    cols = slice(0, h_ref.shape[2])
    part = dot(native(h_ref, cols), dv_ref[...], TN)
    part = (part + dot(native(got_ref, cols), dv_got_ref[...], TN)).astype(BF16)
    half = part.shape[0] // 2
    for p in range(3):

        @pl.when(pl.program_id(0) == p)
        def _():
            outs[2 * p][...] = part[:half]
            outs[2 * p + 1][...] = part[half:]


def plus_kernel(one_ref, two_ref, three_ref, four_ref, top_ref, bottom_ref):
    top_ref[...] = (one_ref[...].astype(F32) + two_ref[...].astype(F32)).astype(BF16)
    bottom_ref[...] = (three_ref[...].astype(F32) + four_ref[...].astype(F32)).astype(BF16)


def join_kernel(top_refs, bottom_refs, out_ref):
    tiles, _, span = out_ref.shape
    half = top_refs[0].shape[0]
    for refs, start in ((top_refs, 0), (bottom_refs, half)):
        total = refs[0][...].astype(F32) + refs[1][...].astype(F32)
        total = (total + refs[2][...].astype(F32)).astype(BF16)
        for t in range(tiles):
            out_ref[t, start : start + half] = total[:, t * span : (t + 1) * span]


def join_parts(*refs):
    join_kernel(refs[:3], refs[3:6], refs[6])


def hold(order_ref, h_ref, held, base):
    shard = h_ref.shape[2] // 8

    @pl.when(pl.program_id(0) == 0)
    def _():
        for p in range(held.shape[1] // shard):
            start = pl.multiple_of(order_ref[base + p] * shard, shard)
            cols = h_ref[:, :, pl.ds(start, shard)].reshape(ROWS, shard)
            held[:, p * shard : (p + 1) * shard] = cols


def near_kernel(order_ref, h_ref, *refs):
    *pieces, sum_ref, held = refs
    hold(order_ref, h_ref, held, 0)
    weight = jnp.concatenate([ref[...] for ref in pieces], axis=0)
    sum_ref[...] = dot(held[...], weight, NN)


def project_kernel(order_ref, h_ref, sum_ref, k_dec_ref, *refs):
    *pieces, v_ref, delta_ref, held = refs
    first = first_rows(DK)
    hold(order_ref, h_ref, held, 6)
    weight = jnp.concatenate([ref[...] for ref in pieces], axis=0)
    v_all = (sum_ref[...] + dot(held[...], weight, NN)).astype(BF16)
    v_ref[...] = v_all
    for j in range(PAIR):
        keys, vals = head_slices(j)
        delta = dot(v_all[:, vals], halves(k_dec_ref[:, keys], first), TN)
        for s in range(SEQS):
            delta_ref[s, j] = delta[:, s * DK : (s + 1) * DK].astype(BF16)


def hidden_grad_kernel(order_ref, dv_ref, *refs):
    *pieces, out_ref = refs
    shard = out_ref.shape[2] // 2
    core = order_ref[0] % 2

    def emit(side, weight):
        grad = dot(dv_ref[...], weight, NT).astype(BF16)
        start = pl.multiple_of(side * shard, shard)
        out_ref[:, :, pl.ds(start, shard)] = grad.reshape(BLK, SEQS, shard)

    groups = (
        ((0,), (5,)),
        ((1, 2), (6, 7)),
        ((3, 4), (8, 9)),
        ((10, 11), (12, 13)),
    )
    for k, (mine, got) in enumerate(groups):

        @pl.when(pl.program_id(0) == k)
        def _():
            emit(core, jnp.concatenate([pieces[n][...] for n in mine], axis=0))
            emit(1 - core, jnp.concatenate([pieces[n][...] for n in got], axis=0))


def final_kernel(
    k_ref,
    g_ref,
    bias_ref,
    cum_ref,
    q_dec_ref,
    do_ref,
    v_ref,
    state_ref,
    dstate_ref,
    dq_ref,
    dk_ref,
    dg_ref,
):
    keep = causal()
    first = first_rows(DK)
    row, col = iota_pair((ROWS, ROWS))
    same = ((row - col) & 1) == 0
    sums = jnp.concatenate(
        [(same & (col >= row)).astype(BF16), (same & (col < row)).astype(BF16)], axis=1
    )
    for j in range(PAIR):
        keys, vals = head_slices(j)
        cum = cum_ref[:, keys]
        last = last_of(cum, first)
        q_scale = SCALE * jnp.exp(cum)
        inv_scale = jnp.exp(-cum)
        dec_scale = jnp.exp(last - cum)
        k = native(k_ref, keys).astype(F32)
        q_dec = q_dec_ref[:, keys]
        k_inv = (k * inv_scale).astype(BF16)
        k_dec = (k * dec_scale).astype(BF16)
        do = native(do_ref, vals)
        v = v_ref[:, vals]
        state = jnp.concatenate([state_ref[0, j], state_ref[1, j]], axis=1)
        dstate = jnp.concatenate([dstate_ref[0, j], dstate_ref[1, j]], axis=1)
        dscores = jnp.where(keep, dot(do, v, NT), 0.0).astype(BF16)
        dq_dec = dot(dscores, k_inv, NN) + chosen(dot(do, state, NN), first)
        dk_inv = dot(dscores, q_dec, TN)
        dk_dec = chosen(dot(v, dstate, NN), first)
        put(dq_ref, keys, (q_scale * dq_dec).astype(BF16))
        dk = (inv_scale * dk_inv + dec_scale * dk_dec).astype(BF16)
        put(dk_ref, keys, dk)
        after = q_dec.astype(F32) * dq_dec - k_inv.astype(F32) * dk_inv
        before = k_dec.astype(F32) * dk_dec
        terms = jnp.concatenate([after, before], axis=0)
        dlog = dot(sums, jnp.concatenate(split2(terms), axis=1), NN)
        through = jnp.sum(state.astype(F32) * dstate.astype(F32), axis=0, keepdims=True)
        through = jnp.where(first, through[:, :DK], through[:, DK:])
        dlog = dlog[:, :DK] + dlog[:, DK:] + jnp.exp(last) * through
        x = native(g_ref, keys).astype(F32) + bias_ref[:, keys]
        slope = (1.0 / SOFTNESS) / (1.0 + jnp.exp(x))
        put(dg_ref, keys, (dlog * slope).astype(BF16))


def over_sp(value):
    return lax.all_to_all(value, "sp", split_axis=0, concat_axis=0, tiled=True)


def shaped(shape, dtype=BF16):
    return jax.ShapeDtypeStruct(shape, dtype)


def arranged(hidden_in, query_act, key_act, gate_act, decay_bias, value_weight, out_grad):
    _, sequences, width = hidden_in.shape
    blocks = lax.axis_size("sp")
    group = lax.axis_size("dp")
    place = lax.axis_index("dp")
    chip, core = place // 2, place % 2
    chips = group // 2
    shard = width // group
    shift = jnp.array([0, -1, 1, 0, -1, 1, 2, 2, 2, 1, -1, 0, 2, 1, -1, 0], jnp.int32)
    other = jnp.array([0, 0, 0, 1, 1, 1, 0, 1, 0, 0, 0, 0, 0, 0, 0, 0], jnp.int32)
    twice = jnp.array([2] * 12 + [1] * 4, jnp.int32)
    order = twice * ((chip + shift + chips) % chips) + (twice - 1) * ((core + other) % 2)
    order = order.astype(jnp.int32)

    def along(value, step):
        pairs = [(d, (d + 2 * step) % group) for d in range(group)]
        return lax.ppermute(value, "dp", pairs)

    def swap(value):
        return lax.ppermute(value, "dp", [(d, d ^ 1) for d in range(group)])

    half = shard // 2
    top, bottom = value_weight[:half], value_weight[half:]

    before_top = along(top, 1)
    after_bottom = along(bottom, -1)
    before_bottom = along(bottom, 1)
    after_top = along(top, -1)
    far_one = along(before_top, 1)
    far_two = along(after_bottom, -1)

    near = [value_weight, before_top, before_bottom, after_top, after_bottom]
    near += [swap(value) for value in near]
    far = [far_one, far_two]
    far += [swap(far_one), swap(far_two)]
    items = sequences * HEADS
    values = HEADS * DV
    bias = decay_bias.reshape(1, HEADS * DK)

    raw_key = pl.BlockSpec((BLK, SEQS, PAIR * DK), lambda i: (0, 0, i))
    raw_val = pl.BlockSpec((BLK, SEQS, PAIR * DV), lambda i: (0, 0, i))
    bias_spec = pl.BlockSpec((1, PAIR * DK), lambda i: (0, i))
    key_spec = pl.BlockSpec((ROWS, PAIR * DK), lambda i: (0, i))
    val_spec = pl.BlockSpec((ROWS, PAIR * DV), lambda i: (0, i))
    state_spec = pl.BlockSpec((SEQS, PAIR, DV, DK), lambda i: (0, i, 0, 0))
    score_spec = pl.BlockSpec((PAIR, ROWS, ROWS), lambda i: (i, 0, 0))
    raw_key_shape = (BLK, SEQS, HEADS * DK)
    key_shape = (ROWS, HEADS * DK)
    val_shape = (ROWS, values)
    state_shape = (SEQS, HEADS, DV, DK)
    mm = 2 * BLK * DK * DV * items
    big = 2 * ROWS * width * values

    delta = pl.pallas_call(
        decay_kernel,
        grid=(STEPS,),
        in_specs=[raw_key, raw_key, bias_spec, raw_val],
        out_specs=pl.BlockSpec((SEQS, PAIR, DV + EXTRA, DK), lambda i: (0, i, 0, 0)),
        out_shape=shaped((SEQS, HEADS, DV + EXTRA, DK)),
        compiler_params=params(),
        cost_estimate=cost(3 * mm, 4 << 20),
        name="decay",
    )(query_act, gate_act, bias, out_grad)

    rx = over_sp(delta.reshape(items, DV + EXTRA, DK))

    cum, q_dec, scores, k_dec = pl.pallas_call(
        intra_kernel,
        grid=(STEPS,),
        in_specs=[raw_key, raw_key, raw_key, bias_spec],
        out_specs=[key_spec, key_spec, score_spec, key_spec],
        out_shape=[
            shaped(key_shape, F32),
            shaped(key_shape),
            shaped((HEADS, ROWS, ROWS)),
            shaped(key_shape),
        ],
        compiler_params=params(),
        cost_estimate=cost(3 * mm, 5 << 20),
        name="intra",
    )(query_act, key_act, gate_act, bias)

    got = swap(hidden_in)

    def scan(arrived, reverse):
        return pl.pallas_call(
            functools.partial(scan_kernel, blocks, reverse),
            out_shape=shaped((blocks, DV, DK)),
            compiler_params=pltpu.CompilerParams(vmem_limit_bytes=12 << 20),
            cost_estimate=cost(mm, 3 << 20),
            name="scan",
        )(arrived, rx)

    dcarried = scan(rx, True)
    dstate = over_sp(dcarried).reshape(state_shape)

    dv = pl.pallas_call(
        value_grad_kernel,
        grid=(STEPS,),
        in_specs=[score_spec, raw_val, key_spec, state_spec],
        out_specs=val_spec,
        out_shape=shaped(val_shape),
        compiler_params=params(),
        cost_estimate=cost(3 * mm, 5 << 20),
        name="value_grad",
    )(scores, out_grad, k_dec, dstate)

    dv_got = swap(dv)
    turns = 2

    def part():
        raw = (BLK, SEQS, shard)
        return pl.pallas_call(
            part_kernel,
            grid_spec=pltpu.PrefetchScalarGridSpec(
                num_scalar_prefetch=1,
                grid=(turns,),
                in_specs=[
                    pl.BlockSpec(raw, lambda i, o: (0, 0, o[8])),
                    pl.BlockSpec(raw, lambda i, o: (0, 0, o[8])),
                    pl.BlockSpec((ROWS, values // turns), lambda i, o: (0, i)),
                    pl.BlockSpec((ROWS, values // turns), lambda i, o: (0, i)),
                ],
                out_specs=[pl.BlockSpec((half, values // turns), lambda i, o: (0, i))] * 2,
            ),
            out_shape=[shaped((half, values))] * 2,
            compiler_params=params(),
            cost_estimate=cost(big // 4, 5 << 20),
        )(order, hidden_in, got, dv, dv_got)

    def rest():
        raw = (BLK, SEQS, shard)
        whole = pl.BlockSpec((ROWS, values), lambda i, o: (0, 0))
        return pl.pallas_call(
            rest_kernel,
            grid_spec=pltpu.PrefetchScalarGridSpec(
                num_scalar_prefetch=1,
                grid=(3,),
                in_specs=[
                    pl.BlockSpec(raw, lambda i, o: (0, 0, o[9 + i])),
                    pl.BlockSpec(raw, lambda i, o: (0, 0, o[9 + i])),
                    whole,
                    whole,
                ],
                out_specs=[pl.BlockSpec((half, values), lambda i, o: (0, 0))] * 6,
            ),
            out_shape=[shaped((half, values))] * 6,
            compiler_params=params(),
            cost_estimate=cost(3 * big // 4, 8 << 20),
            name="part_rest",
        )(order, hidden_in, got, dv, dv_got)

    far_top, far_bottom = part()
    from_before = along(far_top, 1)
    from_after = along(far_bottom, -1)
    next_top, next_bottom, last_top, last_bottom, own_top, own_bottom = rest()
    ready_before = along(next_bottom, 1)
    ready_after = along(last_top, -1)

    late_top, late_bottom = pl.pallas_call(
        plus_kernel,
        out_shape=[shaped((half, values))] * 2,
        compiler_params=pltpu.CompilerParams(vmem_limit_bytes=12 << 20),
        cost_estimate=cost(1 << 22, 3 << 20),
        name="plus",
    )(next_top, from_before, last_bottom, from_after)
    late_before = along(late_top, 1)
    late_after = along(late_bottom, -1)
    partial = pl.pallas_call(
        join_parts,
        out_shape=shaped((blocks, shard, values // blocks)),
        compiler_params=pltpu.CompilerParams(vmem_limit_bytes=20 << 20),
        cost_estimate=cost(1 << 22, 4 << 20),
        name="join",
    )(own_top, late_before, ready_after, own_bottom, ready_before, late_after)

    hidden_spec = pl.BlockSpec((BLK, SEQS, width), lambda i, o: (0, 0, 0))
    wide = pl.BlockSpec((ROWS, PAIR * DV), lambda i, o: (0, i))
    near_spec = pl.BlockSpec((shard, PAIR * DV), lambda i, o: (0, i))
    far_spec = pl.BlockSpec((half, PAIR * DV), lambda i, o: (0, i))
    near_sum = pl.pallas_call(
        near_kernel,
        grid_spec=pltpu.PrefetchScalarGridSpec(
            num_scalar_prefetch=1,
            grid=(STEPS,),
            in_specs=[hidden_spec] + ([near_spec] + [far_spec] * 4) * 2,
            out_specs=wide,
            scratch_shapes=[pltpu.VMEM((ROWS, 6 * shard), BF16)],
        ),
        out_shape=shaped(val_shape, F32),
        compiler_params=params(),
        cost_estimate=cost(3 * big // 4, 10 << 20),
        name="project_near",
    )(order, hidden_in, *near)

    v, vdelta = pl.pallas_call(
        project_kernel,
        grid_spec=pltpu.PrefetchScalarGridSpec(
            num_scalar_prefetch=1,
            grid=(STEPS,),
            in_specs=[
                hidden_spec,
                wide,
                pl.BlockSpec((ROWS, PAIR * DK), lambda i, o: (0, i)),
            ]
            + [far_spec] * 4,
            out_specs=[
                wide,
                pl.BlockSpec((SEQS, PAIR, DV, DK), lambda i, o: (0, i, 0, 0)),
            ],
            scratch_shapes=[pltpu.VMEM((ROWS, 2 * shard), BF16)],
        ),
        out_shape=[shaped(val_shape), shaped(state_shape)],
        compiler_params=params(),
        cost_estimate=cost(big // 4 + mm, 7 << 20),
        name="project",
    )(order, hidden_in, near_sum, k_dec, *far)

    vrx = over_sp(vdelta.reshape(items, DV, DK))
    state = over_sp(scan(vrx, False)).reshape(state_shape)

    whole = pl.BlockSpec((shard, values), lambda i, o: (0, 0))
    part_whole = pl.BlockSpec((half, values), lambda i, o: (0, 0))
    hidden_grad = pl.pallas_call(
        hidden_grad_kernel,
        grid_spec=pltpu.PrefetchScalarGridSpec(
            num_scalar_prefetch=1,
            grid=(chips,),
            in_specs=[pl.BlockSpec(val_shape, lambda i, o: (0, 0))]
            + ([whole] + [part_whole] * 4) * 2
            + [part_whole] * 4,
            out_specs=pl.BlockSpec((BLK, SEQS, 2 * shard), lambda i, o: (0, 0, o[15 - i])),
        ),
        out_shape=shaped((BLK, SEQS, width)),
        compiler_params=params(),
        cost_estimate=cost(big, 10 << 20),
        name="hidden_grad",
    )(order, dv, *near, *far)

    dq, dk, dg = pl.pallas_call(
        final_kernel,
        grid=(STEPS,),
        in_specs=[
            raw_key,
            raw_key,
            bias_spec,
            key_spec,
            key_spec,
            raw_val,
            val_spec,
            state_spec,
            state_spec,
        ],
        out_specs=[raw_key, raw_key, raw_key],
        out_shape=[shaped(raw_key_shape)] * 3,
        compiler_params=params(),
        cost_estimate=cost(6 * mm, 10 << 20),
        name="final",
    )(key_act, gate_act, bias, cum, q_dec, out_grad, v, state, dstate)

    weight_grad = jnp.sum(over_sp(partial).astype(F32), axis=0)
    return (hidden_grad, dq, dk, dg, weight_grad)


def solution(mesh):
    rows = P("sp", "dp", None)
    return jax.shard_map(
        arranged,
        mesh=mesh,
        in_specs=(rows, rows, rows, rows, P(), P("dp", None), rows),
        out_specs=(rows, rows, rows, rows, P("dp", "sp")),
        check_vma=False,
    )
```
